512 devices in a mesh: grp: 2 (over y), fs: 64 (over z, core), tp: 4 (over x).
Axes of the slice: x: 4, y: 2, z: 32, core: 2. Of those that a mesh axis runs over, the one named last changes fastest.
The devices are a block of a 4x8x32 slice.
Arguments:
- tokens: bfloat16 [28672, 2048], P(('grp', 'fs'), 'tp'), parts along dimension 0, may hold values from -6 to 6
- route_ids: int32 [28672, 2], P(('grp', 'fs')), parts along dimension 0, may hold values from 0 to 63, all different within a row; in each aligned block of 224 rows (0 to 223, 224 to 447, ...) at most 10 rows name the same one
- route_weights: float32 [28672, 2], P(('grp', 'fs')), parts along dimension 0, may hold values from 0.25 to 1
- norm_gain: float32 [2048], P('fs'), may hold values from 0.1 to 1.9
- gate_master: float32 [64, 2048, 512], P(None, 'fs', 'tp'), may hold values from -0.125 to 0.125
- up_master: float32 [64, 2048, 512], P(None, 'fs', 'tp'), may hold values from -0.125 to 0.125
- down_master: float32 [64, 2048, 512], P(None, 'fs', 'tp'), may hold values from -0.25 to 0.25
Outputs:
- gate_serve: bfloat16 [128, 2048, 512], P(('grp', 'fs'), None, 'tp'), parts along dimension 0
- up_serve: bfloat16 [128, 2048, 512], P(('grp', 'fs'), None, 'tp'), parts along dimension 0
- down_serve: bfloat16 [128, 2048, 512], P(('grp', 'fs'), None, 'tp'), parts along dimension 0
- moe_output: bfloat16 [28672, 2048], P(('grp', 'fs'), 'tp'), parts along dimension 0
The draws below stay inside these ranges and needn't reach their ends.
There are 2 independent parts, one for each index of `grp`. The reference program is written for one: setup_inputs(seed, part) draws one part's arguments, and reference() takes and returns one part's arrays. A program takes and returns all parts, laid end to end along the dimension named above; an argument that names none is the same for every part. Nothing has to cross between parts.
Inputs may be any that keep to these rules, and one draw needn't show every extreme that they name: `route_ids`: the 2 experts of a row differ; within the rows of one index of fs (aligned blocks of 224 rows) no expert is named more than 10 times.
All inputs are finite; a program needn't handle non-finite values.
Results may differ from the reference program's by a relative error of at most 0.012.
Values may be sent and summed in bfloat16 or wider, within the bound.
A program may use at most 64 MiB of HBM per device.

```python
import math
import jax
import jax.numpy as jnp
import numpy as np
from jax import lax

D = 2048
F = 512
TOP = 2
TOK_DEV = 224
EXPERTS = 64
TOKENS = 14336
CAP = 10
N_FS = 64
N_TP = 4


def block_levels(stream_key, extent, split, smallest, top_value):
    def one(dim, shards_of):
        steps = jax.random.uniform(jax.random.fold_in(jax.random.fold_in(stream_key, 6), dim), (shards_of,), jnp.float32, smallest / len(split), top_value / len(split))
        return jnp.repeat(jnp.exp(steps), extent[dim] // shards_of).reshape((-1,) + (1,) * (len(extent) - dim - 1))

    level = one(*split[0])
    for cut in split[1:]:
        level = level * one(*cut)
    return level


def deal_out(stream_key, own, number, rows, number_of, top, bound, lean):
    ranking = jax.random.permutation(stream_key, number_of)
    crowded, ordinary = portions_of(number_of, rows * top, bound, lean, True), portions_of(number_of, rows * top, bound, lean, False)
    places = jnp.arange(number_of)

    def named(sizes, turn):
        used = int((sizes > 0).sum())
        fixed = max(1, used // 4)
        passed = fixed + (places - fixed + turn * (used - fixed)) % max(1, number_of - fixed)
        return jnp.zeros((number_of,), jnp.int32).at[ranking[jnp.where(places < fixed, places, passed)]].set(jnp.asarray(sizes, jnp.int32))

    sizes = jnp.where(number % 4 == 0, named(crowded, number // 4), named(ordinary, number - number // 4 - 1))
    mixed = jax.random.permutation(jax.random.fold_in(own, 3), number_of)
    donor, taker = mixed[0:number_of // 2 * 2:2], mixed[1:number_of // 2 * 2:2]
    margin = jnp.minimum(sizes[donor] - 1, bound - sizes[taker]) // 2
    margin = jnp.where((donor == ranking[0]) | (taker == ranking[0]) | (sizes[taker] == 0), 0, jnp.maximum(margin, 0))
    passed = jax.random.randint(jax.random.fold_in(own, 4), (number_of // 2,), 0, 1 << 20) % (margin + 1)
    sizes = sizes.at[donor].add(-passed).at[taker].add(passed)
    members = jnp.searchsorted(jnp.cumsum(sizes), jnp.arange(rows * top), side="right").astype(jnp.int32)
    listing = members.reshape(top, rows).T
    listing = listing[jax.random.permutation(jax.random.fold_in(own, 1), rows)]
    turn = jax.random.randint(jax.random.fold_in(own, 2), (rows, 1), 0, top)
    return jnp.take_along_axis(listing, (jnp.arange(top)[None, :] + turn) % top, axis=1)


def portions_of(number_of, total, limit, slope, full):
    loads = [(1 << 20) // math.isqrt(rank ** slope) + 1 for rank in range(1, number_of + 1)]
    largest = limit if full else min(limit, max(-(-total // number_of), total * loads[0] // sum(loads)))
    least = 1 if total - largest >= number_of - 1 else 0
    counts, spare = [largest] + [least] * (number_of - 1), total - largest - least * (number_of - 1)
    while spare > 0:
        candidates = [i for i in range(1, number_of) if counts[i] < largest] or [i for i in range(1, number_of) if counts[i] < limit]
        mass, budget = sum([loads[i] for i in candidates]), spare
        for i in candidates:
            more = min(limit - counts[i], max(1, budget * loads[i] // mass), spare)
            counts[i] = counts[i] + more
            spare = spare - more
    return np.array(counts)


def centred(rng, shape, deviation, limit, cuts=(), kind=jnp.bfloat16):
    values = deviation * jax.random.normal(rng, shape, jnp.float32)
    if cuts:
        values = values * block_levels(rng, shape, cuts, -0.22, 0.18)
    return jnp.clip(values, -limit, limit).astype(kind)


def setup_inputs(seed: int = 0, part: int = 0) -> dict:
    key_list = jax.random.split(jax.random.key(seed), 8)
    part_splits = jax.random.split(jax.random.fold_in(key_list[7], part), 8)
    tokens = centred(part_splits[0], (TOKENS, D), 1.0, 6.0, ((0, 64), (1, 4)))
    route_ids_keys = jax.random.split(jax.random.fold_in(part_splits[1], 1), TOKENS // TOK_DEV)
    route_ids_turns = jax.random.permutation(jax.random.fold_in(part_splits[1], 3), TOKENS // TOK_DEV)
    route_ids = jax.vmap(lambda own, number: deal_out(jax.random.fold_in(part_splits[1], 2), own, number, TOK_DEV, EXPERTS, TOP, CAP, 1))(route_ids_keys, route_ids_turns).reshape((TOKENS, TOP))
    route_weights = jnp.clip(0.25 + 0.75 * jax.random.uniform(part_splits[2], (TOKENS, TOP), jnp.float32) ** block_levels(part_splits[2], (TOKENS, TOP), ((0, 64),), -0.2, 0.2), 0.25, 1.0)
    norm_gain = jnp.clip(1.0 + 0.18 * jax.random.normal(key_list[3], (D,), jnp.float32), 0.1, 1.9)
    gate_master = centred(key_list[4], (EXPERTS, D, F), D ** -0.5, 0.125, ((1, 64), (2, 4)), jnp.float32)
    up_master = centred(key_list[5], (EXPERTS, D, F), D ** -0.5, 0.125, ((1, 64), (2, 4)), jnp.float32)
    down_master = centred(key_list[6], (EXPERTS, D, F), F ** -0.5, 0.25, ((1, 64), (2, 4)), jnp.float32)
    return {"tokens": tokens, "route_ids": route_ids, "route_weights": route_weights, "norm_gain": norm_gain, "gate_master": gate_master, "up_master": up_master, "down_master": down_master}


norm_epsilon = 1e-06

def slot_numbers(route_ids, experts, capacity):
    flat_ids = route_ids.reshape(-1)
    onehot = (flat_ids[:, None] == jnp.arange(experts, dtype=jnp.int32)[None, :]).astype(jnp.int32)
    before = jnp.cumsum(onehot, axis=0) - onehot
    position = lax.optimization_barrier(jnp.sum(before * onehot, axis=1))
    return (flat_ids * capacity + position).astype(jnp.int32).reshape(route_ids.shape)

def reference(tokens, route_ids, route_weights, norm_gain, gate_master, up_master, down_master):
    row_gain = norm_gain[None, :, None]
    gate_serve = (gate_master * row_gain).astype(jnp.bfloat16)
    up_serve = (up_master * row_gain).astype(jnp.bfloat16)
    down_serve = down_master.astype(jnp.bfloat16)
    values = tokens.astype(jnp.float32)
    normed = (values * lax.rsqrt(lax.optimization_barrier(jnp.mean(values * values, axis=1, keepdims=True)) + norm_epsilon)).astype(jnp.bfloat16)
    blocks = normed.reshape(N_FS, TOK_DEV, D)
    expert_ids = route_ids.reshape(N_FS, TOK_DEV, TOP).astype(jnp.int32)
    slot_ids = jax.vmap(lambda ids: slot_numbers(ids, EXPERTS, CAP))(expert_ids)
    block_index = jnp.broadcast_to(jnp.arange(N_FS, dtype=jnp.int32)[:, None, None], slot_ids.shape)
    token_rows = jnp.broadcast_to(blocks[:, :, None, :], (N_FS, TOK_DEV, TOP, D))
    buffer = jnp.zeros((N_FS, EXPERTS * CAP, D), jnp.bfloat16).at[block_index, slot_ids].set(token_rows)
    by_expert = jnp.moveaxis(buffer.reshape(N_FS, EXPERTS, CAP, D), 1, 0)

    def expert_out(inputs):
        rows, gate_w, up_w, down_w = inputs
        flat_rows = rows.reshape(N_FS * CAP, D)
        gate_sum = jnp.dot(flat_rows, gate_w, preferred_element_type=jnp.float32)
        up_sum = jnp.dot(flat_rows, up_w, preferred_element_type=jnp.float32)
        hidden = (jax.nn.silu(gate_sum) * up_sum).astype(jnp.bfloat16)
        parts_hidden = hidden.astype(jnp.float32).reshape(N_FS * CAP, N_TP, F // N_TP)
        parts_down = down_w.astype(jnp.float32).reshape(D, N_TP, F // N_TP)
        partial_value = jnp.einsum('rpf,dpf->prd', parts_hidden, parts_down)
        rounded = lax.optimization_barrier(partial_value.astype(jnp.bfloat16)).astype(jnp.float32)
        return lax.optimization_barrier(jnp.sum(rounded, axis=0)).astype(jnp.bfloat16).reshape(N_FS, CAP, D)
    outputs = lax.map(expert_out, (by_expert, gate_serve, up_serve, down_serve))
    position = slot_ids - expert_ids * CAP
    picked = outputs[expert_ids, block_index, position]
    weights = route_weights.reshape(N_FS, TOK_DEV, TOP)[..., None]
    combined = lax.optimization_barrier(jnp.sum(weights * picked.astype(jnp.float32), axis=2))
    return (gate_serve, up_serve, down_serve, combined.reshape(TOKENS, D).astype(jnp.bfloat16))
```

```python
import functools

import jax
import jax.numpy as jnp
from jax import lax
from jax.experimental import pallas as pl
from jax.experimental.pallas import tpu as pltpu
from jax.sharding import PartitionSpec as P

MESH = pl.DeviceIdType.MESH
GRP_FS = ("grp", "fs")
norm_epsilon = 1e-06

LANES = 128
MAIN = 8
TAIL = 2
RANGES = 8
PAIRS = RANGES // 2

f32, bf16 = jnp.float32, jnp.bfloat16


def iota(shape, dim):
    return lax.broadcasted_iota(jnp.int32, shape, dim)


def ones_where(mask):
    return jnp.where(mask, 1.0, 0.0).astype(bf16)


def drain(ref, sem):
    pltpu.make_async_copy(ref, ref, sem).wait()


def dot(a, b, dims=((1,), (0,))):
    return lax.dot_general(a, b, (dims, ((), ())), preferred_element_type=f32)


def flat(tiles):
    n = tiles.shape[0]
    return tiles.astype(f32).reshape(n * MAIN, LANES)


def kernel(
    shards, columns, groups,
    tok, ids, route_w, gain, gate_m, up_m, down_m,
    out_gate, out_up, out_down, out_moe,
    stage, ws, w, wgu, wd, dx, normed, x, gx, lhs, hb, ob, ret, acc, sq, sq_in,
    stage_sem, out_sem, w_send, w_recv, y_send, y_recv, sq_send, sq_recv, d_send, d_recv,
    xf_send, x_recv, dx_send, dx_recv, h_send, h_recv, r_send, r_recv,
):
    S, T, G = shards, columns, groups
    me, tp, grp = lax.axis_index("fs"), lax.axis_index("tp"), lax.axis_index("grp")
    rs = S // RANGES
    rows, width = tok.shape
    chunks = width // LANES
    depth = gate_m.shape[1]
    mine = lax.rem(me, G) == grp

    def fs_peer(r):
        return {"fs": lax.rem(me + r, S)}

    def tp_peer(j):
        return {"tp": lax.rem(tp + j, T)}

    def grp_peer(j):
        return {"grp": lax.rem(grp + j, G)}

    def remote(src, dst, send, recv, peer):
        return pltpu.make_async_remote_copy(
            src_ref=src, dst_ref=dst, send_sem=send, recv_sem=recv, device_id=peer, device_id_type=MESH
        )

    @pl.when(mine)
    def _():
        for a, ref in enumerate((gate_m, up_m, down_m)):
            pltpu.make_async_copy(ref, stage.at[a], stage_sem.at[a]).start()

    barrier = pltpu.get_barrier_semaphore()

    def greet(r, c):
        pl.semaphore_signal(barrier, inc=1, device_id=fs_peer(r), device_id_type=MESH)
        return c

    lax.fori_loop(1, S, greet, 0)
    for j in range(1, T):
        pl.semaphore_signal(barrier, inc=1, device_id=tp_peer(j), device_id_type=MESH)
    for j in range(1, G):
        pl.semaphore_signal(barrier, inc=1, device_id=grp_peer(j), device_id_type=MESH)

    expert_lane = iota((rows, S), 1)
    rel = []
    for k in range(2):
        r = ids[:, k : k + 1] - me
        rel.append(jnp.where(r < 0, r + S, r))
    named = [jnp.where(r == expert_lane, 1.0, 0.0) for r in rel]
    earlier = ones_where(iota((rows, rows), 0) > iota((rows, rows), 1))
    before = dot(earlier, (named[0] + named[1]).astype(bf16))
    diagonal = iota((rows, rows), 0) == iota((rows, rows), 1)
    main, tail, main_row, tail_row = [], [], [], []
    for k in range(2):
        place = jnp.sum(before * named[k], axis=1, keepdims=True)
        base = rel[k].astype(f32) * MAIN
        main.append(jnp.where(place < MAIN, base + place, -1.0))
        tail.append(jnp.where(place < MAIN, -64.0, base + (place - MAIN)))
        main_row.append(jnp.sum(jnp.where(diagonal, main[k], 0.0), axis=0, keepdims=True))
        tail_row.append(jnp.sum(jnp.where(diagonal, tail[k], 0.0), axis=0, keepdims=True))

    values = tok[...].astype(f32)
    squares = jnp.sum(values * values, axis=1, keepdims=True)
    padded = sq.shape[1]
    spread = iota((rows, padded), 0) == iota((rows, padded), 1)
    as_row = jnp.sum(jnp.where(spread, squares, 0.0), axis=0, keepdims=True)
    sq[...] = jnp.broadcast_to(as_row, sq.shape)

    @pl.when(mine)
    def _():
        for a in range(3):
            drain(stage.at[a], stage_sem.at[a])
        eye = iota((depth, depth), 0) == iota((depth, depth), 1)
        column = jnp.sum(jnp.where(eye, gain[...], 0.0), axis=1, keepdims=True)
        scale = jnp.broadcast_to(column, (depth, LANES))

        def convert(r, c):
            e = lax.rem(me + r, S)
            ws[r, 0] = (stage[0, e] * scale).astype(bf16)
            ws[r, 1] = (stage[1, e] * scale).astype(bf16)
            ws[r, 2] = stage[2, e].astype(bf16)
            return c

        lax.fori_loop(0, S, convert, 0)

    pl.semaphore_wait(barrier, (S - 1) + (T - 1) + (G - 1))

    for j in range(1, T):
        remote(sq, sq_in.at[j - 1], sq_send, sq_recv.at[j - 1], tp_peer(j)).start()

    def far_first(i):
        half = (i + 1) // 2
        return S // 2 + half * (2 * lax.rem(i, 2) - 1)

    w_mine = w.at[:, me // G, lax.rem(me, G)]

    @pl.when(mine)
    def _():
        pltpu.make_async_copy(ws.at[0], w_mine, w_recv).start()

        def ship(i, c):
            r = far_first(i)
            remote(ws.at[r], w_mine, w_send, w_recv, fs_peer(r)).start()
            return c

        lax.fori_loop(0, S - 1, ship, 0)

    total = as_row
    for j in range(1, T):
        drain(sq_in.at[j - 1], sq_recv.at[j - 1])
        total = total + sq_in[j - 1][0:1, :]
    squares = jnp.sum(jnp.where(spread, total, 0.0), axis=1, keepdims=True)
    inverse = lax.rsqrt(squares * (1.0 / (width * T)) + norm_epsilon)
    normed[...] = (values * inverse).astype(bf16)
    slot_row = iota((S * MAIN, rows), 0).astype(f32)
    placing = ones_where((slot_row == main_row[0]) | (slot_row == main_row[1]))
    for c in range(chunks):
        y = dot(placing, normed[:, c * LANES : (c + 1) * LANES])
        x[:, c] = y.reshape(S, MAIN, LANES).astype(bf16)
    y = jnp.zeros((S * MAIN, LANES), f32)
    for c in range(chunks):
        here = slot_row - float(TAIL * c)
        placing = ones_where((here == tail_row[0]) | (here == tail_row[1]))
        y = y + dot(placing, normed[:, c * LANES : (c + 1) * LANES])
    x[:, chunks] = y.reshape(S, MAIN, LANES).astype(bf16)

    pltpu.make_async_copy(x.at[0], gx.at[tp, 0], d_recv.at[0]).start()

    def dispatch(i, c):
        r = far_first(i)
        d = S - r
        remote(x.at[r], gx.at[tp, d], d_send, d_recv.at[d // rs], fs_peer(r)).start()
        return c

    lax.fori_loop(0, S - 1, dispatch, 0)

    def ranges_of(p):
        return (PAIRS - 1 - p, PAIRS + p)

    def forward(p):
        for q in ranges_of(p):
            part = pl.ds(q * rs, rs)
            drain(gx.at[tp, part], d_recv.at[q])
            for j in range(1, T):
                remote(gx.at[tp, part], gx.at[tp, part], xf_send, x_recv.at[p], tp_peer(j)).start()

    drain(w.at[:, :, grp], w_recv)
    for j in range(1, G):
        remote(w.at[:, :, grp], w.at[:, :, grp], y_send, y_recv.at[j - 1], grp_peer(j)).start()
    forward(0)
    for j in range(1, G):
        drain(w.at[:, :, lax.rem(grp + G - j, G)], y_recv.at[j - 1])
    strip = S // T // G
    pltpu.make_async_copy(w.at[2, pl.ds(tp * strip, strip)], dx.at[tp], dx_recv).start()
    for j in range(1, T):
        there = lax.rem(tp + j, T)
        remote(w.at[2, pl.ds(there * strip, strip)], dx.at[tp], dx_send, dx_recv, tp_peer(j)).start()
    outs = (out_gate, out_up, out_down)
    for a, ref in enumerate(outs):
        pltpu.make_async_copy(w.at[a], ref, out_sem.at[a]).start()
    wgu[:, :LANES] = w[0].reshape(S * depth, LANES)
    wgu[:, LANES:] = w[1].reshape(S * depth, LANES)
    drain(dx, dx_recv)
    for j in range(T):
        wd[:, j * LANES : (j + 1) * LANES] = dx[j].reshape(width, LANES)

    half = rs * MAIN
    n_main, n_tail = 2 * half, 2 * rs * TAIL
    q_of = iota((n_tail, n_main), 0)
    tail_home = (q_of >> 1) * MAIN + (q_of & 1)
    picks = [ones_where(iota((n_tail, n_main), 1) == tail_home + TAIL * c) for c in range(chunks)]
    q_of = iota((n_main, n_tail), 1)
    tail_home = (q_of >> 1) * MAIN + (q_of & 1)
    puts = [ones_where(iota((n_main, n_tail), 0) == tail_home + TAIL * c) for c in range(chunks)]

    def first_half(p):
        drain(gx.at[pl.ds(0, T - 1), pl.ds(0, 2 * rs)], x_recv.at[p])
        for j in range(T):
            for s, q in enumerate(ranges_of(p)):
                part = slice(q * rs, (q + 1) * rs)
                for c in range(chunks):
                    k = j * chunks + c
                    lhs[s * half : (s + 1) * half, k * LANES : (k + 1) * LANES] = flat(gx[j, part, c]).astype(bf16)
            tails = jnp.concatenate(
                [flat(gx[j, q * rs : (q + 1) * rs, chunks]) for q in ranges_of(p)], axis=0
            ).astype(bf16)
            for c in range(chunks):
                k = j * chunks + c
                lhs[n_main:, k * LANES : (k + 1) * LANES] = dot(picks[c], tails).astype(bf16)
        both = dot(lhs[...], wgu[...])
        gate, up = both[:, :LANES], both[:, LANES:]
        hb[p, tp] = (gate / (1.0 + jnp.exp(-gate)) * up).astype(bf16)
        for j in range(1, T):
            remote(hb.at[p, tp], hb.at[p, tp], h_send, h_recv.at[p], tp_peer(j)).start()

    def send_back(d):
        back = lax.rem(S - d, S)
        remote(ob.at[d], ret.at[back], r_send, r_recv.at[back // rs], fs_peer(d)).start()

    def second_half(p):
        drain(hb.at[p, pl.ds(0, T - 1)], h_recv.at[p])
        hidden = jnp.concatenate([hb[p, j] for j in range(T)], axis=1)
        o = dot(hidden, wd[...], ((1,), (1,)))
        y = jnp.zeros((n_main, LANES), f32)
        for c in range(chunks):
            lanes = slice(c * LANES, (c + 1) * LANES)
            y = y + dot(puts[c], o[n_main:, lanes].astype(bf16))
        for s, q in enumerate(ranges_of(p)):
            part = slice(q * rs, (q + 1) * rs)
            for c in range(chunks):
                lanes = slice(c * LANES, (c + 1) * LANES)
                ob[part, c] = o[s * half : (s + 1) * half, lanes].reshape(rs, MAIN, LANES).astype(bf16)
            ob[part, chunks] = y[s * half : (s + 1) * half].reshape(rs, MAIN, LANES).astype(bf16)
        near, far = ranges_of(p)

        def send(i, c):
            send_back(far * rs + i)
            send_back(near * rs + rs - 1 - i)
            return c

        if near:
            lax.fori_loop(0, rs, send, 0)
        else:
            lax.fori_loop(0, rs - 1, send, 0)
            send_back(far * rs + rs - 1)
            pltpu.make_async_copy(ob.at[0], ret.at[0], r_recv.at[0]).start()

    for p in range(PAIRS):
        first_half(p)
        if p + 1 < PAIRS:
            forward(p + 1)
        second_half(p)

    acc[...] = jnp.zeros_like(acc)
    for p in range(PAIRS):
        near, far = ranges_of(p)
        lane = iota((rows, n_main), 1)
        home = jnp.where(lane < half, lane + near * half, lane + (far - 1) * half).astype(f32)
        for q in (near, far):
            drain(ret.at[pl.ds(q * rs, rs)], r_recv.at[q])

        def piece(c):
            return jnp.concatenate(
                [flat(ret[q * rs : (q + 1) * rs, c]) for q in (near, far)], axis=0
            ).astype(bf16)

        tails = piece(chunks)
        for c in range(chunks):
            lanes = slice(c * LANES, (c + 1) * LANES)
            values = piece(c)
            for k in range(2):
                acc[k, :, lanes] += dot(ones_where(home == main[k]), values) + dot(
                    ones_where(home == tail[k] + float(TAIL * c)), tails
                )
    out_moe[...] = (route_w[:, 0:1] * acc[0] + route_w[:, 1:2] * acc[1]).astype(bf16)

    drain(sq_in, sq_send)

    @pl.when(mine)
    def _():
        drain(ws.at[pl.ds(1, S - 1)], w_send)

    drain(x.at[pl.ds(1, S - 1)], d_send)
    drain(w.at[:, :, pl.ds(0, G - 1)], y_send)
    drain(gx.at[pl.ds(0, T - 1)], xf_send)
    drain(dx.at[pl.ds(0, T - 1)], dx_send)
    drain(hb.at[:, pl.ds(0, T - 1)], h_send)
    drain(ob.at[pl.ds(1, S - 1)], r_send)
    for a, ref in enumerate(outs):
        drain(w.at[a], out_sem.at[a])


def local(shards, columns, groups, tokens, route_ids, route_weights, norm_gain, gate_m, up_m, down_m):
    S, T, G = shards, columns, groups
    rows, width = tokens.shape
    depth = gate_m.shape[1]
    chunks = width // LANES
    rs = S // RANGES
    padded = -(-rows // LANES) * LANES
    n_rows = 2 * rs * (MAIN + TAIL)
    vmem = pl.BlockSpec(memory_space=pltpu.VMEM)
    anywhere = pl.BlockSpec(memory_space=pl.ANY)
    dma = pltpu.SemaphoreType.DMA
    block = (chunks + 1, MAIN, LANES)
    served = jax.ShapeDtypeStruct((S // G, G, depth, LANES), bf16)
    outs = pl.pallas_call(
        functools.partial(kernel, S, T, G),
        out_shape=(served, served, served, jax.ShapeDtypeStruct((rows, width), bf16)),
        in_specs=[vmem] * 4 + [anywhere] * 3,
        out_specs=(anywhere, anywhere, anywhere, vmem),
        scratch_shapes=[
            pltpu.VMEM((3, S, depth, LANES), f32),
            pltpu.VMEM((S, 3, depth, LANES), bf16),
            pltpu.VMEM((3, S // G, G, depth, LANES), bf16),
            pltpu.VMEM((S * depth, 2 * LANES), bf16),
            pltpu.VMEM((width, T * LANES), bf16),
            pltpu.VMEM((T, S // T // G, G, depth, LANES), bf16),
            pltpu.VMEM((rows, width), bf16),
            pltpu.VMEM((S, *block), bf16),
            pltpu.VMEM((T, S, *block), bf16),
            pltpu.VMEM((n_rows, T * width), bf16),
            pltpu.VMEM((PAIRS, T, n_rows, LANES), bf16),
            pltpu.VMEM((S, *block), bf16),
            pltpu.VMEM((S, *block), bf16),
            pltpu.VMEM((2, rows, width), f32),
            pltpu.VMEM((MAIN, padded), f32),
            pltpu.VMEM((T - 1, MAIN, padded), f32),
            dma((3,)), dma((3,)), dma, dma, dma, dma((max(G - 1, 1),)), dma, dma((T - 1,)), dma, dma((RANGES,)),
            dma, dma((PAIRS,)), dma, dma, dma, dma((PAIRS,)), dma, dma((RANGES,)),
        ],
        compiler_params=pltpu.CompilerParams(collective_id=0, has_side_effects=True),
    )(tokens, route_ids, route_weights, norm_gain[None, :], gate_m, up_m, down_m)
    gate, up, down = (o.reshape(1, S * depth, LANES) for o in outs[:3])
    return gate, up, down, outs[3]


def solution(mesh):
    placed = (
        P(GRP_FS, "tp"), P(GRP_FS, None), P(GRP_FS, None), P("fs"),
        P(None, "fs", "tp"), P(None, "fs", "tp"), P(None, "fs", "tp"),
    )
    return jax.shard_map(
        functools.partial(local, mesh.shape["fs"], mesh.shape["tp"], mesh.shape["grp"]),
        mesh=mesh,
        in_specs=placed,
        out_specs=(P(GRP_FS, None, "tp"), P(GRP_FS, None, "tp"), P(GRP_FS, None, "tp"), P(GRP_FS, "tp")),
        check_vma=False,
    )
```

```python
import functools

import jax
import jax.numpy as jnp
from jax import lax
from jax.experimental import pallas as pl
from jax.experimental.pallas import tpu as pltpu
from jax.sharding import PartitionSpec as P

MESH = pl.DeviceIdType.MESH
GRP_FS = ("grp", "fs")
norm_epsilon = 1e-06

LANES = 128
MAIN = 8
TAIL = 2
RANGES = 8
PAIRS = RANGES // 2

f32, bf16 = jnp.float32, jnp.bfloat16


def iota(shape, dim):
    return lax.broadcasted_iota(jnp.int32, shape, dim)


def ones_where(mask):
    return jnp.where(mask, 1.0, 0.0).astype(bf16)


def drain(ref, sem):
    pltpu.make_async_copy(ref, ref, sem).wait()


def dot(a, b, dims=((1,), (0,))):
    return lax.dot_general(a, b, (dims, ((), ())), preferred_element_type=f32)


def flat(tiles):
    n = tiles.shape[0]
    return tiles.astype(f32).reshape(n * MAIN, LANES)


def kernel(
    shards, columns, groups,
    tok, ids, route_w, gain, gate_m, up_m, down_m,
    out_gate, out_up, out_down, out_moe,
    stage, ws, w, wgu, wd, dx, normed, x, gx, lhs, hb, ob, ret, acc, sq, sq_in, ready,
    stage_sem, out_sem, w_send, w_recv, y_send, y_recv, sq_send, sq_recv, d_send, d_recv,
    xf_send, x_recv, dx_send, dx_recv, h_send, h_recv, r_send, r_recv,
):
    S, T, G = shards, columns, groups
    me, tp, grp = lax.axis_index("fs"), lax.axis_index("tp"), lax.axis_index("grp")
    rs = S // RANGES
    rows, width = tok.shape
    chunks = width // LANES
    depth = gate_m.shape[1]
    mine = lax.rem(me, G) == grp

    def fs_peer(r):
        return {"fs": lax.rem(me + r, S)}

    def tp_peer(j):
        return {"tp": lax.rem(tp + j, T)}

    def grp_peer(j):
        return {"grp": lax.rem(grp + j, G)}

    def remote(src, dst, send, recv, peer):
        return pltpu.make_async_remote_copy(
            src_ref=src, dst_ref=dst, send_sem=send, recv_sem=recv, device_id=peer, device_id_type=MESH
        )

    @pl.when(mine)
    def _():
        for a, ref in enumerate((gate_m, up_m, down_m)):
            pltpu.make_async_copy(ref, stage.at[a], stage_sem.at[a]).start()

    place_of = lax.rem(me + S - 1, S)

    def placed_at(q):
        return {"fs": lax.rem(q + 1, S)}

    barrier = pltpu.get_barrier_semaphore()
    for j in range(1, T):
        pl.semaphore_signal(barrier, inc=1, device_id=tp_peer(j), device_id_type=MESH)
    for j in range(1, G):
        pl.semaphore_signal(barrier, inc=1, device_id=grp_peer(j), device_id_type=MESH)
    pl.semaphore_wait(barrier, (T - 1) + (G - 1) + (place_of + S - 1) // S)

    @pl.when(place_of < S - 1)
    def _():
        pl.semaphore_signal(barrier, inc=1, device_id=placed_at(place_of + 1), device_id_type=MESH)

    def report(q, c):
        pl.semaphore_signal(ready.at[place_of], inc=1, device_id=placed_at(q), device_id_type=MESH)
        return c

    lax.fori_loop(0, place_of, report, 0)

    w_mine = w.at[:, me // G, lax.rem(me, G)]

    def ship(q):
        r = lax.rem(q + 1 + S - me, S)
        remote(ws.at[r], w_mine, w_send, w_recv, placed_at(q)).start()

    @pl.when(mine)
    def _():
        for a in range(3):
            drain(stage.at[a], stage_sem.at[a])
        eye = iota((depth, depth), 0) == iota((depth, depth), 1)
        column = jnp.sum(jnp.where(eye, gain[...], 0.0), axis=1, keepdims=True)
        scale = jnp.broadcast_to(column, (depth, LANES))

        def convert(r, c):
            e = lax.rem(me + r, S)
            ws[r, 0] = (stage[0, e] * scale).astype(bf16)
            ws[r, 1] = (stage[1, e] * scale).astype(bf16)
            ws[r, 2] = stage[2, e].astype(bf16)
            return c

        lax.fori_loop(0, S, convert, 0)
        pltpu.make_async_copy(ws.at[0], w_mine, w_recv).start()

        def ship_before(i, c):
            odd = lax.rem(i, 2)
            ship(odd * (i // 2) + (1 - odd) * (place_of - 1 - i // 2))
            return c

        lax.fori_loop(0, place_of, ship_before, 0)

    expert_lane = iota((rows, S), 1)
    rel = []
    for k in range(2):
        r = ids[:, k : k + 1] - me
        rel.append(jnp.where(r < 0, r + S, r))
    named = [jnp.where(r == expert_lane, 1.0, 0.0) for r in rel]
    earlier = ones_where(iota((rows, rows), 0) > iota((rows, rows), 1))
    before = dot(earlier, (named[0] + named[1]).astype(bf16))
    diagonal = iota((rows, rows), 0) == iota((rows, rows), 1)
    main, tail, main_row, tail_row = [], [], [], []
    for k in range(2):
        place = jnp.sum(before * named[k], axis=1, keepdims=True)
        base = rel[k].astype(f32) * MAIN
        main.append(jnp.where(place < MAIN, base + place, -1.0))
        tail.append(jnp.where(place < MAIN, -64.0, base + (place - MAIN)))
        main_row.append(jnp.sum(jnp.where(diagonal, main[k], 0.0), axis=0, keepdims=True))
        tail_row.append(jnp.sum(jnp.where(diagonal, tail[k], 0.0), axis=0, keepdims=True))

    values = tok[...].astype(f32)
    squares = jnp.sum(values * values, axis=1, keepdims=True)
    padded = sq.shape[1]
    spread = iota((rows, padded), 0) == iota((rows, padded), 1)
    as_row = jnp.sum(jnp.where(spread, squares, 0.0), axis=0, keepdims=True)
    sq[...] = jnp.broadcast_to(as_row, sq.shape)

    for j in range(1, T):
        remote(sq, sq_in.at[j - 1], sq_send, sq_recv.at[j - 1], tp_peer(j)).start()

    def far_first(i):
        half = (i + 1) // 2
        return S // 2 + half * (2 * lax.rem(i, 2) - 1)

    total = as_row
    for j in range(1, T):
        drain(sq_in.at[j - 1], sq_recv.at[j - 1])
        total = total + sq_in[j - 1][0:1, :]
    squares = jnp.sum(jnp.where(spread, total, 0.0), axis=1, keepdims=True)
    inverse = lax.rsqrt(squares * (1.0 / (width * T)) + norm_epsilon)
    normed[...] = (values * inverse).astype(bf16)
    slot_row = iota((S * MAIN, rows), 0).astype(f32)
    placing = ones_where((slot_row == main_row[0]) | (slot_row == main_row[1]))
    for c in range(chunks):
        y = dot(placing, normed[:, c * LANES : (c + 1) * LANES])
        x[:, c] = y.reshape(S, MAIN, LANES).astype(bf16)
    y = jnp.zeros((S * MAIN, LANES), f32)
    for c in range(chunks):
        here = slot_row - float(TAIL * c)
        placing = ones_where((here == tail_row[0]) | (here == tail_row[1]))
        y = y + dot(placing, normed[:, c * LANES : (c + 1) * LANES])
    x[:, chunks] = y.reshape(S, MAIN, LANES).astype(bf16)

    def ship_after(q, c):
        pl.semaphore_wait(ready.at[q], 1)

        @pl.when(mine)
        def _():
            ship(q)

        return c

    lax.fori_loop(place_of + 1, S, ship_after, 0)

    pltpu.make_async_copy(x.at[0], gx.at[tp, 0], d_recv.at[0]).start()

    def dispatch(i, c):
        r = far_first(i)
        d = S - r
        remote(x.at[r], gx.at[tp, d], d_send, d_recv.at[d // rs], fs_peer(r)).start()
        return c

    lax.fori_loop(0, S - 1, dispatch, 0)

    def ranges_of(p):
        return (PAIRS - 1 - p, PAIRS + p)

    def forward(p):
        for q in ranges_of(p):
            part = pl.ds(q * rs, rs)
            drain(gx.at[tp, part], d_recv.at[q])
            for j in range(1, T):
                remote(gx.at[tp, part], gx.at[tp, part], xf_send, x_recv.at[p], tp_peer(j)).start()

    drain(w.at[:, :, grp], w_recv)
    for j in range(1, G):
        remote(w.at[:, :, grp], w.at[:, :, grp], y_send, y_recv.at[j - 1], grp_peer(j)).start()
    forward(0)
    for j in range(1, G):
        drain(w.at[:, :, lax.rem(grp + G - j, G)], y_recv.at[j - 1])
    strip = S // T // G
    pltpu.make_async_copy(w.at[2, pl.ds(tp * strip, strip)], dx.at[tp], dx_recv).start()
    for j in range(1, T):
        there = lax.rem(tp + j, T)
        remote(w.at[2, pl.ds(there * strip, strip)], dx.at[tp], dx_send, dx_recv, tp_peer(j)).start()
    outs = (out_gate, out_up, out_down)
    for a, ref in enumerate(outs):
        pltpu.make_async_copy(w.at[a], ref, out_sem.at[a]).start()
    wgu[:, :LANES] = w[0].reshape(S * depth, LANES)
    wgu[:, LANES:] = w[1].reshape(S * depth, LANES)
    drain(dx, dx_recv)
    for j in range(T):
        wd[:, j * LANES : (j + 1) * LANES] = dx[j].reshape(width, LANES)

    half = rs * MAIN
    n_main, n_tail = 2 * half, 2 * rs * TAIL
    q_of = iota((n_tail, n_main), 0)
    tail_home = (q_of >> 1) * MAIN + (q_of & 1)
    picks = [ones_where(iota((n_tail, n_main), 1) == tail_home + TAIL * c) for c in range(chunks)]
    q_of = iota((n_main, n_tail), 1)
    tail_home = (q_of >> 1) * MAIN + (q_of & 1)
    puts = [ones_where(iota((n_main, n_tail), 0) == tail_home + TAIL * c) for c in range(chunks)]

    def first_half(p):
        drain(gx.at[pl.ds(0, T - 1), pl.ds(0, 2 * rs)], x_recv.at[p])
        for j in range(T):
            for s, q in enumerate(ranges_of(p)):
                part = slice(q * rs, (q + 1) * rs)
                for c in range(chunks):
                    k = j * chunks + c
                    lhs[s * half : (s + 1) * half, k * LANES : (k + 1) * LANES] = flat(gx[j, part, c]).astype(bf16)
            tails = jnp.concatenate(
                [flat(gx[j, q * rs : (q + 1) * rs, chunks]) for q in ranges_of(p)], axis=0
            ).astype(bf16)
            for c in range(chunks):
                k = j * chunks + c
                lhs[n_main:, k * LANES : (k + 1) * LANES] = dot(picks[c], tails).astype(bf16)
        both = dot(lhs[...], wgu[...])
        gate, up = both[:, :LANES], both[:, LANES:]
        hb[p, tp] = (gate / (1.0 + jnp.exp(-gate)) * up).astype(bf16)
        for j in range(1, T):
            remote(hb.at[p, tp], hb.at[p, tp], h_send, h_recv.at[p], tp_peer(j)).start()

    def send_back(d):
        back = lax.rem(S - d, S)
        remote(ob.at[d], ret.at[back], r_send, r_recv.at[back // rs], fs_peer(d)).start()

    def second_half(p):
        drain(hb.at[p, pl.ds(0, T - 1)], h_recv.at[p])
        hidden = jnp.concatenate([hb[p, j] for j in range(T)], axis=1)
        o = dot(hidden, wd[...], ((1,), (1,)))
        y = jnp.zeros((n_main, LANES), f32)
        for c in range(chunks):
            lanes = slice(c * LANES, (c + 1) * LANES)
            y = y + dot(puts[c], o[n_main:, lanes].astype(bf16))
        for s, q in enumerate(ranges_of(p)):
            part = slice(q * rs, (q + 1) * rs)
            for c in range(chunks):
                lanes = slice(c * LANES, (c + 1) * LANES)
                ob[part, c] = o[s * half : (s + 1) * half, lanes].reshape(rs, MAIN, LANES).astype(bf16)
            ob[part, chunks] = y[s * half : (s + 1) * half].reshape(rs, MAIN, LANES).astype(bf16)
        near, far = ranges_of(p)

        def send(i, c):
            send_back(far * rs + i)
            send_back(near * rs + rs - 1 - i)
            return c

        if near:
            lax.fori_loop(0, rs, send, 0)
        else:
            lax.fori_loop(0, rs - 1, send, 0)
            send_back(far * rs + rs - 1)
            pltpu.make_async_copy(ob.at[0], ret.at[0], r_recv.at[0]).start()

    for p in range(PAIRS):
        first_half(p)
        if p + 1 < PAIRS:
            forward(p + 1)
        second_half(p)

    acc[...] = jnp.zeros_like(acc)
    for p in range(PAIRS):
        near, far = ranges_of(p)
        lane = iota((rows, n_main), 1)
        home = jnp.where(lane < half, lane + near * half, lane + (far - 1) * half).astype(f32)
        for q in (near, far):
            drain(ret.at[pl.ds(q * rs, rs)], r_recv.at[q])

        def piece(c):
            return jnp.concatenate(
                [flat(ret[q * rs : (q + 1) * rs, c]) for q in (near, far)], axis=0
            ).astype(bf16)

        tails = piece(chunks)
        for c in range(chunks):
            lanes = slice(c * LANES, (c + 1) * LANES)
            values = piece(c)
            for k in range(2):
                acc[k, :, lanes] += dot(ones_where(home == main[k]), values) + dot(
                    ones_where(home == tail[k] + float(TAIL * c)), tails
                )
    out_moe[...] = (route_w[:, 0:1] * acc[0] + route_w[:, 1:2] * acc[1]).astype(bf16)

    drain(sq_in, sq_send)

    @pl.when(mine)
    def _():
        drain(ws.at[pl.ds(1, S - 1)], w_send)

    drain(x.at[pl.ds(1, S - 1)], d_send)
    drain(w.at[:, :, pl.ds(0, G - 1)], y_send)
    drain(gx.at[pl.ds(0, T - 1)], xf_send)
    drain(dx.at[pl.ds(0, T - 1)], dx_send)
    drain(hb.at[:, pl.ds(0, T - 1)], h_send)
    drain(ob.at[pl.ds(1, S - 1)], r_send)
    for a, ref in enumerate(outs):
        drain(w.at[a], out_sem.at[a])


def local(shards, columns, groups, tokens, route_ids, route_weights, norm_gain, gate_m, up_m, down_m):
    S, T, G = shards, columns, groups
    rows, width = tokens.shape
    depth = gate_m.shape[1]
    chunks = width // LANES
    rs = S // RANGES
    padded = -(-rows // LANES) * LANES
    n_rows = 2 * rs * (MAIN + TAIL)
    vmem = pl.BlockSpec(memory_space=pltpu.VMEM)
    anywhere = pl.BlockSpec(memory_space=pl.ANY)
    dma = pltpu.SemaphoreType.DMA
    block = (chunks + 1, MAIN, LANES)
    served = jax.ShapeDtypeStruct((S // G, G, depth, LANES), bf16)
    outs = pl.pallas_call(
        functools.partial(kernel, S, T, G),
        out_shape=(served, served, served, jax.ShapeDtypeStruct((rows, width), bf16)),
        in_specs=[vmem] * 4 + [anywhere] * 3,
        out_specs=(anywhere, anywhere, anywhere, vmem),
        scratch_shapes=[
            pltpu.VMEM((3, S, depth, LANES), f32),
            pltpu.VMEM((S, 3, depth, LANES), bf16),
            pltpu.VMEM((3, S // G, G, depth, LANES), bf16),
            pltpu.VMEM((S * depth, 2 * LANES), bf16),
            pltpu.VMEM((width, T * LANES), bf16),
            pltpu.VMEM((T, S // T // G, G, depth, LANES), bf16),
            pltpu.VMEM((rows, width), bf16),
            pltpu.VMEM((S, *block), bf16),
            pltpu.VMEM((T, S, *block), bf16),
            pltpu.VMEM((n_rows, T * width), bf16),
            pltpu.VMEM((PAIRS, T, n_rows, LANES), bf16),
            pltpu.VMEM((S, *block), bf16),
            pltpu.VMEM((S, *block), bf16),
            pltpu.VMEM((2, rows, width), f32),
            pltpu.VMEM((MAIN, padded), f32),
            pltpu.VMEM((T - 1, MAIN, padded), f32),
            pltpu.SemaphoreType.REGULAR((S,)),
            dma((3,)), dma((3,)), dma, dma, dma, dma((max(G - 1, 1),)), dma, dma((T - 1,)), dma, dma((RANGES,)),
            dma, dma((PAIRS,)), dma, dma, dma, dma((PAIRS,)), dma, dma((RANGES,)),
        ],
        compiler_params=pltpu.CompilerParams(collective_id=0, has_side_effects=True),
    )(tokens, route_ids, route_weights, norm_gain[None, :], gate_m, up_m, down_m)
    gate, up, down = (o.reshape(1, S * depth, LANES) for o in outs[:3])
    return gate, up, down, outs[3]


def solution(mesh):
    placed = (
        P(GRP_FS, "tp"), P(GRP_FS, None), P(GRP_FS, None), P("fs"),
        P(None, "fs", "tp"), P(None, "fs", "tp"), P(None, "fs", "tp"),
    )
    return jax.shard_map(
        functools.partial(local, mesh.shape["fs"], mesh.shape["tp"], mesh.shape["grp"]),
        mesh=mesh,
        in_specs=placed,
        out_specs=(P(GRP_FS, None, "tp"), P(GRP_FS, None, "tp"), P(GRP_FS, None, "tp"), P(GRP_FS, "tp")),
        check_vma=False,
    )
```

```python
import functools

import jax
import jax.numpy as jnp
from jax import lax
from jax.experimental import pallas as pl
from jax.experimental.pallas import tpu as pltpu
from jax.sharding import PartitionSpec as P

MESH = pl.DeviceIdType.MESH
GRP_FS = ("grp", "fs")
norm_epsilon = 1e-06

LANES = 128
MAIN = 8
TAIL = 2
RANGES = 8
PAIRS = RANGES // 2

f32, bf16 = jnp.float32, jnp.bfloat16


def iota(shape, dim):
    return lax.broadcasted_iota(jnp.int32, shape, dim)


def ones_where(mask):
    return jnp.where(mask, 1.0, 0.0).astype(bf16)


def drain(ref, sem):
    pltpu.make_async_copy(ref, ref, sem).wait()


def dot(a, b, dims=((1,), (0,))):
    return lax.dot_general(a, b, (dims, ((), ())), preferred_element_type=f32)


def flat(tiles):
    n = tiles.shape[0]
    return tiles.astype(f32).reshape(n * MAIN, LANES)


def kernel(
    shards, columns, groups,
    tok, ids, route_w, gain, gate_m, up_m, down_m,
    out_gate, out_up, out_down, out_moe,
    stage, ws, w, wgu, wd, dx, normed, x, gx, lhs, hb, ob, ret, acc, sq, sq_in, ready,
    stage_sem, out_sem, w_send, w_recv, y_send, y_recv, sq_send, sq_recv, d_send, d_recv,
    xf_send, x_recv, dx_send, dx_recv, h_send, h_recv, r_send, r_recv,
):
    S, T, G = shards, columns, groups
    me, tp, grp = lax.axis_index("fs"), lax.axis_index("tp"), lax.axis_index("grp")
    rs = S // RANGES
    rows, width = tok.shape
    chunks = width // LANES
    depth = gate_m.shape[1]
    mine = lax.rem(me, G) == grp

    def fs_peer(r):
        return {"fs": lax.rem(me + r, S)}

    def tp_peer(j):
        return {"tp": lax.rem(tp + j, T)}

    def grp_peer(j):
        return {"grp": lax.rem(grp + j, G)}

    def remote(src, dst, send, recv, peer):
        return pltpu.make_async_remote_copy(
            src_ref=src, dst_ref=dst, send_sem=send, recv_sem=recv, device_id=peer, device_id_type=MESH
        )

    @pl.when(mine)
    def _():
        for a, ref in enumerate((gate_m, up_m, down_m)):
            pltpu.make_async_copy(ref, stage.at[a], stage_sem.at[a]).start()

    place_of = lax.rem(me + S - 1, S)

    def placed_at(q):
        return {"fs": lax.rem(q + 1, S)}

    barrier = pltpu.get_barrier_semaphore()

    def greet(q, c):
        pl.semaphore_signal(barrier, inc=1, device_id=placed_at(q), device_id_type=MESH)
        return c

    lax.fori_loop(place_of + 1, S, greet, 0)
    for j in range(1, T):
        pl.semaphore_signal(barrier, inc=1, device_id=tp_peer(j), device_id_type=MESH)
    for j in range(1, G):
        pl.semaphore_signal(barrier, inc=1, device_id=grp_peer(j), device_id_type=MESH)
    pl.semaphore_wait(barrier, place_of + (T - 1) + (G - 1))

    def report(q, c):
        pl.semaphore_signal(ready.at[place_of], inc=1, device_id=placed_at(q), device_id_type=MESH)
        return c

    lax.fori_loop(0, place_of, report, 0)

    w_mine = w.at[:, me // G, lax.rem(me, G)]

    def ship(q):
        r = lax.rem(q + 1 + S - me, S)
        remote(ws.at[r], w_mine, w_send, w_recv, placed_at(q)).start()

    @pl.when(mine)
    def _():
        for a in range(3):
            drain(stage.at[a], stage_sem.at[a])
        eye = iota((depth, depth), 0) == iota((depth, depth), 1)
        column = jnp.sum(jnp.where(eye, gain[...], 0.0), axis=1, keepdims=True)
        scale = jnp.broadcast_to(column, (depth, LANES))

        def convert(r, c):
            e = lax.rem(me + r, S)
            ws[r, 0] = (stage[0, e] * scale).astype(bf16)
            ws[r, 1] = (stage[1, e] * scale).astype(bf16)
            ws[r, 2] = stage[2, e].astype(bf16)
            return c

        lax.fori_loop(0, S, convert, 0)
        pltpu.make_async_copy(ws.at[0], w_mine, w_recv).start()

        def ship_before(i, c):
            odd = lax.rem(i, 2)
            ship(odd * (i // 2) + (1 - odd) * (place_of - 1 - i // 2))
            return c

        lax.fori_loop(0, place_of, ship_before, 0)

    diagonal = iota((rows, rows), 0) == iota((rows, rows), 1)

    def as_column(row):
        return jnp.sum(jnp.where(diagonal, row, 0.0), axis=1, keepdims=True)

    expert_lane = iota((rows, S), 1).astype(f32)
    rel = []
    for k in range(2):
        r = ids[k : k + 1, :] - me
        rel.append(as_column(jnp.where(r < 0, r + S, r).astype(f32)))
    named = [jnp.where(r == expert_lane, 1.0, 0.0) for r in rel]
    earlier = ones_where(iota((rows, rows), 0) > iota((rows, rows), 1))
    before = dot(earlier, (named[0] + named[1]).astype(bf16))
    main, tail, main_row, tail_row = [], [], [], []
    for k in range(2):
        place = jnp.sum(before * named[k], axis=1, keepdims=True)
        base = rel[k] * MAIN
        main.append(jnp.where(place < MAIN, base + place, -1.0))
        tail.append(jnp.where(place < MAIN, -64.0, base + (place - MAIN)))
        main_row.append(jnp.sum(jnp.where(diagonal, main[k], 0.0), axis=0, keepdims=True))
        tail_row.append(jnp.sum(jnp.where(diagonal, tail[k], 0.0), axis=0, keepdims=True))

    values = tok[...].astype(f32)
    squares = jnp.sum(values * values, axis=1, keepdims=True)
    padded = sq.shape[1]
    spread = iota((rows, padded), 0) == iota((rows, padded), 1)
    as_row = jnp.sum(jnp.where(spread, squares, 0.0), axis=0, keepdims=True)
    sq[...] = jnp.broadcast_to(as_row, sq.shape)

    for j in range(1, T):
        remote(sq, sq_in.at[j - 1], sq_send, sq_recv.at[j - 1], tp_peer(j)).start()

    def far_first(i):
        half = (i + 1) // 2
        return S // 2 + half * (2 * lax.rem(i, 2) - 1)

    total = as_row
    for j in range(1, T):
        drain(sq_in.at[j - 1], sq_recv.at[j - 1])
        total = total + sq_in[j - 1][0:1, :]
    squares = jnp.sum(jnp.where(spread, total, 0.0), axis=1, keepdims=True)
    inverse = lax.rsqrt(squares * (1.0 / (width * T)) + norm_epsilon)
    normed[...] = (values * inverse).astype(bf16)
    slot_row = iota((S * MAIN, rows), 0).astype(f32)
    placing = ones_where((slot_row == main_row[0]) | (slot_row == main_row[1]))
    for c in range(chunks):
        y = dot(placing, normed[:, c * LANES : (c + 1) * LANES])
        x[:, c] = y.reshape(S, MAIN, LANES).astype(bf16)
    y = jnp.zeros((S * MAIN, LANES), f32)
    for c in range(chunks):
        here = slot_row - float(TAIL * c)
        placing = ones_where((here == tail_row[0]) | (here == tail_row[1]))
        y = y + dot(placing, normed[:, c * LANES : (c + 1) * LANES])
    x[:, chunks] = y.reshape(S, MAIN, LANES).astype(bf16)

    def ship_after(q, c):
        pl.semaphore_wait(ready.at[q], 1)

        @pl.when(mine)
        def _():
            ship(q)

        return c

    lax.fori_loop(place_of + 1, S, ship_after, 0)

    pltpu.make_async_copy(x.at[0], gx.at[tp, 0], d_recv.at[0]).start()

    def dispatch(i, c):
        r = far_first(i)
        d = S - r
        remote(x.at[r], gx.at[tp, d], d_send, d_recv.at[d // rs], fs_peer(r)).start()
        return c

    lax.fori_loop(0, S - 1, dispatch, 0)

    def ranges_of(p):
        return (PAIRS - 1 - p, PAIRS + p)

    def forward(p):
        for q in ranges_of(p):
            part = pl.ds(q * rs, rs)
            drain(gx.at[tp, part], d_recv.at[q])
            for j in range(1, T):
                remote(gx.at[tp, part], gx.at[tp, part], xf_send, x_recv.at[p], tp_peer(j)).start()

    drain(w.at[:, :, grp], w_recv)
    for j in range(1, G):
        remote(w.at[:, :, grp], w.at[:, :, grp], y_send, y_recv.at[j - 1], grp_peer(j)).start()
    forward(0)
    for j in range(1, G):
        drain(w.at[:, :, lax.rem(grp + G - j, G)], y_recv.at[j - 1])
    strip = S // T // G
    pltpu.make_async_copy(w.at[2, pl.ds(tp * strip, strip)], dx.at[tp], dx_recv).start()
    for j in range(1, T):
        there = lax.rem(tp + j, T)
        remote(w.at[2, pl.ds(there * strip, strip)], dx.at[tp], dx_send, dx_recv, tp_peer(j)).start()
    outs = (out_gate, out_up, out_down)
    for a, ref in enumerate(outs):
        pltpu.make_async_copy(w.at[a], ref, out_sem.at[a]).start()
    wgu[:, :LANES] = w[0].reshape(S * depth, LANES)
    wgu[:, LANES:] = w[1].reshape(S * depth, LANES)
    drain(dx, dx_recv)
    for j in range(T):
        wd[:, j * LANES : (j + 1) * LANES] = dx[j].reshape(width, LANES)

    half = rs * MAIN
    n_main, n_tail = 2 * half, 2 * rs * TAIL
    q_of = iota((n_tail, n_main), 0)
    tail_home = (q_of >> 1) * MAIN + (q_of & 1)
    picks = [ones_where(iota((n_tail, n_main), 1) == tail_home + TAIL * c) for c in range(chunks)]
    q_of = iota((n_main, n_tail), 1)
    tail_home = (q_of >> 1) * MAIN + (q_of & 1)
    puts = [ones_where(iota((n_main, n_tail), 0) == tail_home + TAIL * c) for c in range(chunks)]

    def first_half(p):
        drain(gx.at[pl.ds(0, T - 1), pl.ds(0, 2 * rs)], x_recv.at[p])
        for j in range(T):
            for s, q in enumerate(ranges_of(p)):
                part = slice(q * rs, (q + 1) * rs)
                for c in range(chunks):
                    k = j * chunks + c
                    lhs[s * half : (s + 1) * half, k * LANES : (k + 1) * LANES] = flat(gx[j, part, c]).astype(bf16)
            tails = jnp.concatenate(
                [flat(gx[j, q * rs : (q + 1) * rs, chunks]) for q in ranges_of(p)], axis=0
            ).astype(bf16)
            for c in range(chunks):
                k = j * chunks + c
                lhs[n_main:, k * LANES : (k + 1) * LANES] = dot(picks[c], tails).astype(bf16)
        both = dot(lhs[...], wgu[...])
        gate, up = both[:, :LANES], both[:, LANES:]
        hb[p, tp] = (gate / (1.0 + jnp.exp(-gate)) * up).astype(bf16)
        for j in range(1, T):
            remote(hb.at[p, tp], hb.at[p, tp], h_send, h_recv.at[p], tp_peer(j)).start()

    def send_back(d):
        back = lax.rem(S - d, S)
        remote(ob.at[d], ret.at[back], r_send, r_recv.at[back // rs], fs_peer(d)).start()

    def second_half(p):
        drain(hb.at[p, pl.ds(0, T - 1)], h_recv.at[p])
        hidden = jnp.concatenate([hb[p, j] for j in range(T)], axis=1)
        o = dot(hidden, wd[...], ((1,), (1,)))
        y = jnp.zeros((n_main, LANES), f32)
        for c in range(chunks):
            lanes = slice(c * LANES, (c + 1) * LANES)
            y = y + dot(puts[c], o[n_main:, lanes].astype(bf16))
        for s, q in enumerate(ranges_of(p)):
            part = slice(q * rs, (q + 1) * rs)
            for c in range(chunks):
                lanes = slice(c * LANES, (c + 1) * LANES)
                ob[part, c] = o[s * half : (s + 1) * half, lanes].reshape(rs, MAIN, LANES).astype(bf16)
            ob[part, chunks] = y[s * half : (s + 1) * half].reshape(rs, MAIN, LANES).astype(bf16)
        near, far = ranges_of(p)

        def send(i, c):
            send_back(far * rs + i)
            send_back(near * rs + rs - 1 - i)
            return c

        if near:
            lax.fori_loop(0, rs, send, 0)
        else:
            lax.fori_loop(0, rs - 1, send, 0)
            send_back(far * rs + rs - 1)
            pltpu.make_async_copy(ob.at[0], ret.at[0], r_recv.at[0]).start()

    for p in range(PAIRS):
        first_half(p)
        if p + 1 < PAIRS:
            forward(p + 1)
        second_half(p)

    acc[...] = jnp.zeros_like(acc)
    for p in range(PAIRS):
        near, far = ranges_of(p)
        lane = iota((rows, n_main), 1)
        home = jnp.where(lane < half, lane + near * half, lane + (far - 1) * half).astype(f32)
        for q in (near, far):
            drain(ret.at[pl.ds(q * rs, rs)], r_recv.at[q])

        def piece(c):
            return jnp.concatenate(
                [flat(ret[q * rs : (q + 1) * rs, c]) for q in (near, far)], axis=0
            ).astype(bf16)

        tails = piece(chunks)
        for c in range(chunks):
            lanes = slice(c * LANES, (c + 1) * LANES)
            values = piece(c)
            for k in range(2):
                acc[k, :, lanes] += dot(ones_where(home == main[k]), values) + dot(
                    ones_where(home == tail[k] + float(TAIL * c)), tails
                )
    weight = [as_column(route_w[k : k + 1, :]) for k in range(2)]
    out_moe[...] = (weight[0] * acc[0] + weight[1] * acc[1]).astype(bf16)

    drain(sq_in, sq_send)

    @pl.when(mine)
    def _():
        drain(ws.at[pl.ds(1, S - 1)], w_send)

    drain(x.at[pl.ds(1, S - 1)], d_send)
    drain(w.at[:, :, pl.ds(0, G - 1)], y_send)
    drain(gx.at[pl.ds(0, T - 1)], xf_send)
    drain(dx.at[pl.ds(0, T - 1)], dx_send)
    drain(hb.at[:, pl.ds(0, T - 1)], h_send)
    drain(ob.at[pl.ds(1, S - 1)], r_send)
    for a, ref in enumerate(outs):
        drain(w.at[a], out_sem.at[a])


def local(shards, columns, groups, tokens, route_ids, route_weights, norm_gain, gate_m, up_m, down_m):
    S, T, G = shards, columns, groups
    rows, width = tokens.shape
    depth = gate_m.shape[1]
    chunks = width // LANES
    rs = S // RANGES
    padded = -(-rows // LANES) * LANES
    n_rows = 2 * rs * (MAIN + TAIL)
    vmem = pl.BlockSpec(memory_space=pltpu.VMEM)
    anywhere = pl.BlockSpec(memory_space=pl.ANY)
    dma = pltpu.SemaphoreType.DMA
    block = (chunks + 1, MAIN, LANES)
    served = jax.ShapeDtypeStruct((S // G, G, depth, LANES), bf16)
    outs = pl.pallas_call(
        functools.partial(kernel, S, T, G),
        out_shape=(served, served, served, jax.ShapeDtypeStruct((rows, width), bf16)),
        in_specs=[vmem] * 4 + [anywhere] * 3,
        out_specs=(anywhere, anywhere, anywhere, vmem),
        scratch_shapes=[
            pltpu.VMEM((3, S, depth, LANES), f32),
            pltpu.VMEM((S, 3, depth, LANES), bf16),
            pltpu.VMEM((3, S // G, G, depth, LANES), bf16),
            pltpu.VMEM((S * depth, 2 * LANES), bf16),
            pltpu.VMEM((width, T * LANES), bf16),
            pltpu.VMEM((T, S // T // G, G, depth, LANES), bf16),
            pltpu.VMEM((rows, width), bf16),
            pltpu.VMEM((S, *block), bf16),
            pltpu.VMEM((T, S, *block), bf16),
            pltpu.VMEM((n_rows, T * width), bf16),
            pltpu.VMEM((PAIRS, T, n_rows, LANES), bf16),
            pltpu.VMEM((S, *block), bf16),
            pltpu.VMEM((S, *block), bf16),
            pltpu.VMEM((2, rows, width), f32),
            pltpu.VMEM((MAIN, padded), f32),
            pltpu.VMEM((T - 1, MAIN, padded), f32),
            pltpu.SemaphoreType.REGULAR((S,)),
            dma((3,)), dma((3,)), dma, dma, dma, dma((max(G - 1, 1),)), dma, dma((T - 1,)), dma, dma((RANGES,)),
            dma, dma((PAIRS,)), dma, dma, dma, dma((PAIRS,)), dma, dma((RANGES,)),
        ],
        compiler_params=pltpu.CompilerParams(collective_id=0, has_side_effects=True),
    )(tokens, route_ids.T, route_weights.T, norm_gain[None, :], gate_m, up_m, down_m)
    gate, up, down = (o.reshape(1, S * depth, LANES) for o in outs[:3])
    return gate, up, down, outs[3]


def solution(mesh):
    placed = (
        P(GRP_FS, "tp"), P(GRP_FS, None), P(GRP_FS, None), P("fs"),
        P(None, "fs", "tp"), P(None, "fs", "tp"), P(None, "fs", "tp"),
    )
    return jax.shard_map(
        functools.partial(local, mesh.shape["fs"], mesh.shape["tp"], mesh.shape["grp"]),
        mesh=mesh,
        in_specs=placed,
        out_specs=(P(GRP_FS, None, "tp"), P(GRP_FS, None, "tp"), P(GRP_FS, None, "tp"), P(GRP_FS, "tp")),
        check_vma=False,
    )
```

```python
import functools

import jax
import jax.numpy as jnp
from jax import lax
from jax.experimental import pallas as pl
from jax.experimental.pallas import tpu as pltpu
from jax.sharding import PartitionSpec as P

MESH = pl.DeviceIdType.MESH
GRP_FS = ("grp", "fs")
norm_epsilon = 1e-06

LANES = 128
MAIN = 8
TAIL = 2
RANGES = 8
PAIRS = RANGES // 2

f32, bf16 = jnp.float32, jnp.bfloat16


def iota(shape, dim):
    return lax.broadcasted_iota(jnp.int32, shape, dim)


def ones_where(mask):
    return jnp.where(mask, 1.0, 0.0).astype(bf16)


def drain(ref, sem):
    pltpu.make_async_copy(ref, ref, sem).wait()


def parts_of(groups):
    rows = min(groups, 4)
    return groups // rows, rows


def tall(blocks):
    if blocks.shape[-2] % 16:
        return blocks.astype(f32).reshape(-1, LANES).astype(bf16)
    return blocks.reshape(-1, LANES)


def dot(a, b, dims=((1,), (0,))):
    return lax.dot_general(a, b, (dims, ((), ())), preferred_element_type=f32)


def flat(tiles):
    n = tiles.shape[0]
    return tiles.astype(f32).reshape(n * MAIN, LANES)


def kernel(
    shards, columns, groups,
    tok, ids, route_w, gain, gate_m, up_m, down_m,
    out_gate, out_up, out_down, out_moe,
    stage, ws, w, wgu, wd, dx, normed, x, gx, lhs, hb, ob, ret, acc, sq, sq_in, ready,
    stage_sem, out_sem, w_send, w_recv, y_send, y_recv, sq_send, sq_recv, d_send, d_recv,
    xf_send, x_recv, dx_send, dx_recv, h_send, h_recv, r_send, r_recv,
):
    S, T, G = shards, columns, groups
    me, tp, grp = lax.axis_index("fs"), lax.axis_index("tp"), lax.axis_index("grp")
    rs = S // RANGES
    rows, width = tok.shape
    chunks = width // LANES
    depth = gate_m.shape[1]
    Q, R = parts_of(G)
    strip = depth // R
    turn, part = grp // R, lax.rem(grp, R)
    mine = lax.rem(me, Q) == turn

    def fs_peer(r):
        return {"fs": lax.rem(me + r, S)}

    def tp_peer(j):
        return {"tp": lax.rem(tp + j, T)}

    def grp_peer(j):
        return {"grp": lax.rem(grp + j, G)}

    def remote(src, dst, send, recv, peer):
        return pltpu.make_async_remote_copy(
            src_ref=src, dst_ref=dst, send_sem=send, recv_sem=recv, device_id=peer, device_id_type=MESH
        )

    @pl.when(mine)
    def _():
        for a, ref in enumerate((gate_m, up_m, down_m)):
            pltpu.make_async_copy(ref.at[:, pl.ds(part * strip, strip)], stage.at[a], stage_sem.at[a]).start()

    place_of = lax.rem(me + S - 1, S)

    def placed_at(q):
        return {"fs": lax.rem(q + 1, S)}

    barrier = pltpu.get_barrier_semaphore()

    def greet(q, c):
        pl.semaphore_signal(barrier, inc=1, device_id=placed_at(q), device_id_type=MESH)
        return c

    lax.fori_loop(place_of + 1, S, greet, 0)
    for j in range(1, T):
        pl.semaphore_signal(barrier, inc=1, device_id=tp_peer(j), device_id_type=MESH)
    for j in range(1, G):
        pl.semaphore_signal(barrier, inc=1, device_id=grp_peer(j), device_id_type=MESH)
    pl.semaphore_wait(barrier, place_of + (T - 1) + (G - 1))

    def report(q, c):
        pl.semaphore_signal(ready.at[place_of], inc=1, device_id=placed_at(q), device_id_type=MESH)
        return c

    lax.fori_loop(0, place_of, report, 0)

    w_mine = w.at[:, me // Q, lax.rem(me, Q), part]
    w_group = w.at[:, :, turn, part]

    def ship(q):
        r = lax.rem(q + 1 + S - me, S)
        remote(ws.at[r], w_mine, w_send, w_recv, placed_at(q)).start()

    @pl.when(mine)
    def _():
        for a in range(3):
            drain(stage.at[a], stage_sem.at[a])
        eye = iota((strip, depth), 0) + part * strip == iota((strip, depth), 1)
        column = jnp.sum(jnp.where(eye, gain[...], 0.0), axis=1, keepdims=True)
        scale = jnp.broadcast_to(column, (strip, LANES))

        def convert(r, c):
            e = lax.rem(me + r, S)
            ws[r, 0] = (stage[0, e] * scale).astype(bf16)
            ws[r, 1] = (stage[1, e] * scale).astype(bf16)
            ws[r, 2] = stage[2, e].astype(bf16)
            return c

        lax.fori_loop(0, S, convert, 0)
        pltpu.make_async_copy(ws.at[0], w_mine, w_recv).start()

        def ship_before(i, c):
            odd = lax.rem(i, 2)
            ship(odd * (i // 2) + (1 - odd) * (place_of - 1 - i // 2))
            return c

        lax.fori_loop(0, place_of, ship_before, 0)

    diagonal = iota((rows, rows), 0) == iota((rows, rows), 1)

    def as_column(row):
        return jnp.sum(jnp.where(diagonal, row, 0.0), axis=1, keepdims=True)

    expert_lane = iota((rows, S), 1).astype(f32)
    rel = []
    for k in range(2):
        r = ids[k : k + 1, :] - me
        rel.append(as_column(jnp.where(r < 0, r + S, r).astype(f32)))
    named = [jnp.where(r == expert_lane, 1.0, 0.0) for r in rel]
    earlier = ones_where(iota((rows, rows), 0) > iota((rows, rows), 1))
    before = dot(earlier, (named[0] + named[1]).astype(bf16))
    main, tail, main_row, tail_row = [], [], [], []
    for k in range(2):
        place = jnp.sum(before * named[k], axis=1, keepdims=True)
        base = rel[k] * MAIN
        main.append(jnp.where(place < MAIN, base + place, -1.0))
        tail.append(jnp.where(place < MAIN, -64.0, base + (place - MAIN)))
        main_row.append(jnp.sum(jnp.where(diagonal, main[k], 0.0), axis=0, keepdims=True))
        tail_row.append(jnp.sum(jnp.where(diagonal, tail[k], 0.0), axis=0, keepdims=True))

    values = tok[...].astype(f32)
    squares = jnp.sum(values * values, axis=1, keepdims=True)
    padded = sq.shape[1]
    spread = iota((rows, padded), 0) == iota((rows, padded), 1)
    as_row = jnp.sum(jnp.where(spread, squares, 0.0), axis=0, keepdims=True)
    sq[...] = jnp.broadcast_to(as_row, sq.shape)

    for j in range(1, T):
        remote(sq, sq_in.at[j - 1], sq_send, sq_recv.at[j - 1], tp_peer(j)).start()

    def far_first(i):
        half = (i + 1) // 2
        return S // 2 + half * (2 * lax.rem(i, 2) - 1)

    total = as_row
    for j in range(1, T):
        drain(sq_in.at[j - 1], sq_recv.at[j - 1])
        total = total + sq_in[j - 1][0:1, :]
    squares = jnp.sum(jnp.where(spread, total, 0.0), axis=1, keepdims=True)
    inverse = lax.rsqrt(squares * (1.0 / (width * T)) + norm_epsilon)
    normed[...] = (values * inverse).astype(bf16)
    slot_row = iota((S * MAIN, rows), 0).astype(f32)
    placing = ones_where((slot_row == main_row[0]) | (slot_row == main_row[1]))
    for c in range(chunks):
        y = dot(placing, normed[:, c * LANES : (c + 1) * LANES])
        x[:, c] = y.reshape(S, MAIN, LANES).astype(bf16)
    y = jnp.zeros((S * MAIN, LANES), f32)
    for c in range(chunks):
        here = slot_row - float(TAIL * c)
        placing = ones_where((here == tail_row[0]) | (here == tail_row[1]))
        y = y + dot(placing, normed[:, c * LANES : (c + 1) * LANES])
    x[:, chunks] = y.reshape(S, MAIN, LANES).astype(bf16)

    def ship_after(q, c):
        pl.semaphore_wait(ready.at[q], 1)

        @pl.when(mine)
        def _():
            ship(q)

        return c

    lax.fori_loop(place_of + 1, S, ship_after, 0)

    pltpu.make_async_copy(x.at[0], gx.at[tp, 0], d_recv.at[0]).start()

    def dispatch(i, c):
        r = far_first(i)
        d = S - r
        remote(x.at[r], gx.at[tp, d], d_send, d_recv.at[d // rs], fs_peer(r)).start()
        return c

    lax.fori_loop(0, S - 1, dispatch, 0)

    def ranges_of(p):
        return (PAIRS - 1 - p, PAIRS + p)

    def forward(p):
        for q in ranges_of(p):
            part = pl.ds(q * rs, rs)
            drain(gx.at[tp, part], d_recv.at[q])
            for j in range(1, T):
                remote(gx.at[tp, part], gx.at[tp, part], xf_send, x_recv.at[p], tp_peer(j)).start()

    drain(w_group, w_recv)
    for j in range(1, G):
        remote(w_group, w_group, y_send, y_recv.at[j - 1], grp_peer(j)).start()
    forward(0)
    for j in range(1, G):
        other = lax.rem(grp + G - j, G)
        drain(w.at[:, :, other // R, lax.rem(other, R)], y_recv.at[j - 1])
    share = S // T // Q
    pltpu.make_async_copy(w.at[2, pl.ds(tp * share, share)], dx.at[tp], dx_recv).start()
    for j in range(1, T):
        there = lax.rem(tp + j, T)
        remote(w.at[2, pl.ds(there * share, share)], dx.at[tp], dx_send, dx_recv, tp_peer(j)).start()
    outs = (out_gate, out_up, out_down)
    for a, ref in enumerate(outs):
        pltpu.make_async_copy(w.at[a], ref, out_sem.at[a]).start()
    wgu[:, :LANES] = tall(w[0])
    wgu[:, LANES:] = tall(w[1])
    drain(dx, dx_recv)
    for j in range(T):
        wd[:, j * LANES : (j + 1) * LANES] = tall(dx[j])

    half = rs * MAIN
    n_main, n_tail = 2 * half, 2 * rs * TAIL
    q_of = iota((n_tail, n_main), 0)
    tail_home = (q_of >> 1) * MAIN + (q_of & 1)
    picks = [ones_where(iota((n_tail, n_main), 1) == tail_home + TAIL * c) for c in range(chunks)]
    q_of = iota((n_main, n_tail), 1)
    tail_home = (q_of >> 1) * MAIN + (q_of & 1)
    puts = [ones_where(iota((n_main, n_tail), 0) == tail_home + TAIL * c) for c in range(chunks)]

    def first_half(p):
        drain(gx.at[pl.ds(0, T - 1), pl.ds(0, 2 * rs)], x_recv.at[p])
        for j in range(T):
            for s, q in enumerate(ranges_of(p)):
                part = slice(q * rs, (q + 1) * rs)
                for c in range(chunks):
                    k = j * chunks + c
                    lhs[s * half : (s + 1) * half, k * LANES : (k + 1) * LANES] = flat(gx[j, part, c]).astype(bf16)
            tails = jnp.concatenate(
                [flat(gx[j, q * rs : (q + 1) * rs, chunks]) for q in ranges_of(p)], axis=0
            ).astype(bf16)
            for c in range(chunks):
                k = j * chunks + c
                lhs[n_main:, k * LANES : (k + 1) * LANES] = dot(picks[c], tails).astype(bf16)
        both = dot(lhs[...], wgu[...])
        gate, up = both[:, :LANES], both[:, LANES:]
        hb[p, tp] = (gate / (1.0 + jnp.exp(-gate)) * up).astype(bf16)
        for j in range(1, T):
            remote(hb.at[p, tp], hb.at[p, tp], h_send, h_recv.at[p], tp_peer(j)).start()

    def send_back(d):
        back = lax.rem(S - d, S)
        remote(ob.at[d], ret.at[back], r_send, r_recv.at[back // rs], fs_peer(d)).start()

    def second_half(p):
        drain(hb.at[p, pl.ds(0, T - 1)], h_recv.at[p])
        hidden = jnp.concatenate([hb[p, j] for j in range(T)], axis=1)
        o = dot(hidden, wd[...], ((1,), (1,)))
        y = jnp.zeros((n_main, LANES), f32)
        for c in range(chunks):
            lanes = slice(c * LANES, (c + 1) * LANES)
            y = y + dot(puts[c], o[n_main:, lanes].astype(bf16))
        for s, q in enumerate(ranges_of(p)):
            part = slice(q * rs, (q + 1) * rs)
            for c in range(chunks):
                lanes = slice(c * LANES, (c + 1) * LANES)
                ob[part, c] = o[s * half : (s + 1) * half, lanes].reshape(rs, MAIN, LANES).astype(bf16)
            ob[part, chunks] = y[s * half : (s + 1) * half].reshape(rs, MAIN, LANES).astype(bf16)
        near, far = ranges_of(p)

        def send(i, c):
            send_back(far * rs + i)
            send_back(near * rs + rs - 1 - i)
            return c

        if near:
            lax.fori_loop(0, rs, send, 0)
        else:
            lax.fori_loop(0, rs - 1, send, 0)
            send_back(far * rs + rs - 1)
            pltpu.make_async_copy(ob.at[0], ret.at[0], r_recv.at[0]).start()

    for p in range(PAIRS):
        first_half(p)
        if p + 1 < PAIRS:
            forward(p + 1)
        second_half(p)

    acc[...] = jnp.zeros_like(acc)
    for p in range(PAIRS):
        near, far = ranges_of(p)
        lane = iota((rows, n_main), 1)
        home = jnp.where(lane < half, lane + near * half, lane + (far - 1) * half).astype(f32)
        for q in (near, far):
            drain(ret.at[pl.ds(q * rs, rs)], r_recv.at[q])

        def piece(c):
            return jnp.concatenate(
                [flat(ret[q * rs : (q + 1) * rs, c]) for q in (near, far)], axis=0
            ).astype(bf16)

        tails = piece(chunks)
        for c in range(chunks):
            lanes = slice(c * LANES, (c + 1) * LANES)
            values = piece(c)
            for k in range(2):
                acc[k, :, lanes] += dot(ones_where(home == main[k]), values) + dot(
                    ones_where(home == tail[k] + float(TAIL * c)), tails
                )
    weight = [as_column(route_w[k : k + 1, :]) for k in range(2)]
    out_moe[...] = (weight[0] * acc[0] + weight[1] * acc[1]).astype(bf16)

    drain(sq_in, sq_send)

    @pl.when(mine)
    def _():
        drain(ws.at[pl.ds(1, S - 1)], w_send)

    drain(x.at[pl.ds(1, S - 1)], d_send)
    for j in range(1, G):
        drain(w_group, y_send)
    drain(gx.at[pl.ds(0, T - 1)], xf_send)
    drain(dx.at[pl.ds(0, T - 1)], dx_send)
    drain(hb.at[:, pl.ds(0, T - 1)], h_send)
    drain(ob.at[pl.ds(1, S - 1)], r_send)
    for a, ref in enumerate(outs):
        drain(w.at[a], out_sem.at[a])


def local(shards, columns, groups, tokens, route_ids, route_weights, norm_gain, gate_m, up_m, down_m):
    S, T, G = shards, columns, groups
    rows, width = tokens.shape
    depth = gate_m.shape[1]
    chunks = width // LANES
    rs = S // RANGES
    padded = -(-rows // LANES) * LANES
    n_rows = 2 * rs * (MAIN + TAIL)
    vmem = pl.BlockSpec(memory_space=pltpu.VMEM)
    anywhere = pl.BlockSpec(memory_space=pl.ANY)
    dma = pltpu.SemaphoreType.DMA
    block = (chunks + 1, MAIN, LANES)
    Q, R = parts_of(G)
    strip = depth // R
    served = jax.ShapeDtypeStruct((S // Q, Q, R, strip, LANES), bf16)
    outs = pl.pallas_call(
        functools.partial(kernel, S, T, G),
        out_shape=(served, served, served, jax.ShapeDtypeStruct((rows, width), bf16)),
        in_specs=[vmem] * 4 + [anywhere] * 3,
        out_specs=(anywhere, anywhere, anywhere, vmem),
        scratch_shapes=[
            pltpu.VMEM((3, S, strip, LANES), f32),
            pltpu.VMEM((S, 3, strip, LANES), bf16),
            pltpu.VMEM((3, S // Q, Q, R, strip, LANES), bf16),
            pltpu.VMEM((S * depth, 2 * LANES), bf16),
            pltpu.VMEM((width, T * LANES), bf16),
            pltpu.VMEM((T, S // T // Q, Q, R, strip, LANES), bf16),
            pltpu.VMEM((rows, width), bf16),
            pltpu.VMEM((S, *block), bf16),
            pltpu.VMEM((T, S, *block), bf16),
            pltpu.VMEM((n_rows, T * width), bf16),
            pltpu.VMEM((PAIRS, T, n_rows, LANES), bf16),
            pltpu.VMEM((S, *block), bf16),
            pltpu.VMEM((S, *block), bf16),
            pltpu.VMEM((2, rows, width), f32),
            pltpu.VMEM((MAIN, padded), f32),
            pltpu.VMEM((T - 1, MAIN, padded), f32),
            pltpu.SemaphoreType.REGULAR((S,)),
            dma((3,)), dma((3,)), dma, dma, dma, dma((max(G - 1, 1),)), dma, dma((T - 1,)), dma, dma((RANGES,)),
            dma, dma((PAIRS,)), dma, dma, dma, dma((PAIRS,)), dma, dma((RANGES,)),
        ],
        compiler_params=pltpu.CompilerParams(collective_id=0, has_side_effects=True),
    )(tokens, route_ids.T, route_weights.T, norm_gain[None, :], gate_m, up_m, down_m)
    gate, up, down = (o.reshape(1, S * depth, LANES) for o in outs[:3])
    return gate, up, down, outs[3]


def solution(mesh):
    placed = (
        P(GRP_FS, "tp"), P(GRP_FS, None), P(GRP_FS, None), P("fs"),
        P(None, "fs", "tp"), P(None, "fs", "tp"), P(None, "fs", "tp"),
    )
    return jax.shard_map(
        functools.partial(local, mesh.shape["fs"], mesh.shape["tp"], mesh.shape["grp"]),
        mesh=mesh,
        in_specs=placed,
        out_specs=(P(GRP_FS, None, "tp"), P(GRP_FS, None, "tp"), P(GRP_FS, None, "tp"), P(GRP_FS, "tp")),
        check_vma=False,
    )
```

```python
import functools

import jax
import jax.numpy as jnp
from jax import lax
from jax.experimental import pallas as pl
from jax.experimental.pallas import tpu as pltpu
from jax.sharding import PartitionSpec as P

MESH = pl.DeviceIdType.MESH
GRP_FS = ("grp", "fs")
norm_epsilon = 1e-06

LANES = 128
MAIN = 8
TAIL = 2
RANGES = 8
PAIRS = RANGES // 2

f32, bf16 = jnp.float32, jnp.bfloat16


def iota(shape, dim):
    return lax.broadcasted_iota(jnp.int32, shape, dim)


def ones_where(mask):
    return jnp.where(mask, 1.0, 0.0).astype(bf16)


def drain(ref, sem):
    pltpu.make_async_copy(ref, ref, sem).wait()


def parts_of(groups):
    rows = min(groups, 4)
    return groups // rows, rows


def tall(blocks):
    if blocks.shape[-2] % 16:
        return blocks.astype(f32).reshape(-1, LANES).astype(bf16)
    return blocks.reshape(-1, LANES)


def dot(a, b, dims=((1,), (0,))):
    return lax.dot_general(a, b, (dims, ((), ())), preferred_element_type=f32)


def flat(tiles):
    n = tiles.shape[0]
    return tiles.astype(f32).reshape(n * MAIN, LANES)


def kernel(
    shards, columns, groups,
    tok, ids, route_w, gain, gate_m, up_m, down_m,
    out_gate, out_up, out_down, out_moe,
    stage, ws, w, wgu, wd, dx, normed, x, gx, lhs, hb, ob, ret, acc, sq, sq_in, ready,
    stage_sem, out_sem, w_send, w_recv, y_send, y_recv, sq_send, sq_recv, d_send, d_recv,
    xf_send, x_recv, dx_send, dx_recv, h_send, h_recv, r_send, r_recv,
):
    S, T, G = shards, columns, groups
    me, tp, grp = lax.axis_index("fs"), lax.axis_index("tp"), lax.axis_index("grp")
    rs = S // RANGES
    rows, width = tok.shape
    chunks = width // LANES
    depth = gate_m.shape[1]
    Q, R = parts_of(G)
    strip = depth // R
    turn, part = grp // R, lax.rem(grp, R)
    mine = lax.rem(me, Q) == turn

    def fs_peer(r):
        return {"fs": lax.rem(me + r, S)}

    def tp_peer(j):
        return {"tp": lax.rem(tp + j, T)}

    def grp_peer(j):
        return {"grp": lax.rem(grp + j, G)}

    def remote(src, dst, send, recv, peer):
        return pltpu.make_async_remote_copy(
            src_ref=src, dst_ref=dst, send_sem=send, recv_sem=recv, device_id=peer, device_id_type=MESH
        )

    @pl.when(mine)
    def _():
        for a, ref in enumerate((gate_m, up_m, down_m)):
            pltpu.make_async_copy(ref.at[:, pl.ds(part * strip, strip)], stage.at[a], stage_sem.at[a]).start()

    place_of = lax.rem(me + S - 1, S)

    def placed_at(q):
        return {"fs": lax.rem(q + 1, S)}

    barrier = pltpu.get_barrier_semaphore()

    def greet(q, c):
        pl.semaphore_signal(barrier, inc=1, device_id=placed_at(q), device_id_type=MESH)
        return c

    lax.fori_loop(place_of + 1, S, greet, 0)
    for j in range(1, T):
        pl.semaphore_signal(barrier, inc=1, device_id=tp_peer(j), device_id_type=MESH)
    for j in range(1, G):
        pl.semaphore_signal(barrier, inc=1, device_id=grp_peer(j), device_id_type=MESH)
    pl.semaphore_wait(barrier, place_of + (T - 1) + (G - 1))

    def report(q, c):
        pl.semaphore_signal(ready.at[place_of], inc=1, device_id=placed_at(q), device_id_type=MESH)
        return c

    lax.fori_loop(0, place_of, report, 0)

    w_mine = w.at[:, me // Q, lax.rem(me, Q), part]
    w_group = w.at[:, :, turn, part]

    def ship(q):
        r = lax.rem(q + 1 + S - me, S)
        remote(ws.at[r], w_mine, w_send, w_recv, placed_at(q)).start()

    @pl.when(mine)
    def _():
        for a in range(3):
            drain(stage.at[a], stage_sem.at[a])
        eye = iota((strip, depth), 0) + part * strip == iota((strip, depth), 1)
        column = jnp.sum(jnp.where(eye, gain[...], 0.0), axis=1, keepdims=True)
        scale = jnp.broadcast_to(column, (strip, LANES))

        def convert(r, c):
            e = lax.rem(me + r, S)
            ws[r, 0] = (stage[0, e] * scale).astype(bf16)
            ws[r, 1] = (stage[1, e] * scale).astype(bf16)
            ws[r, 2] = stage[2, e].astype(bf16)
            return c

        lax.fori_loop(0, S, convert, 0)
        pltpu.make_async_copy(ws.at[0], w_mine, w_recv).start()

        def ship_before(i, c):
            odd = lax.rem(i, 2)
            ship(odd * (i // 2) + (1 - odd) * (place_of - 1 - i // 2))
            return c

        lax.fori_loop(0, place_of, ship_before, 0)

    diagonal = iota((rows, rows), 0) == iota((rows, rows), 1)

    def as_column(row):
        return jnp.sum(jnp.where(diagonal, row, 0.0), axis=1, keepdims=True)

    expert_lane = iota((rows, S), 1).astype(f32)
    rel = []
    for k in range(2):
        r = ids[k : k + 1, :] - me
        rel.append(as_column(jnp.where(r < 0, r + S, r).astype(f32)))
    named = [jnp.where(r == expert_lane, 1.0, 0.0) for r in rel]
    earlier = ones_where(iota((rows, rows), 0) > iota((rows, rows), 1))
    before = dot(earlier, (named[0] + named[1]).astype(bf16))
    main, tail, main_row, tail_row = [], [], [], []
    for k in range(2):
        place = jnp.sum(before * named[k], axis=1, keepdims=True)
        base = rel[k] * MAIN
        main.append(jnp.where(place < MAIN, base + place, -1.0))
        tail.append(jnp.where(place < MAIN, -64.0, base + (place - MAIN)))
        main_row.append(jnp.sum(jnp.where(diagonal, main[k], 0.0), axis=0, keepdims=True))
        tail_row.append(jnp.sum(jnp.where(diagonal, tail[k], 0.0), axis=0, keepdims=True))

    values = tok[...].astype(f32)
    squares = jnp.sum(values * values, axis=1, keepdims=True)
    padded = sq.shape[1]
    spread = iota((rows, padded), 0) == iota((rows, padded), 1)
    as_row = jnp.sum(jnp.where(spread, squares, 0.0), axis=0, keepdims=True)
    sq[...] = jnp.broadcast_to(as_row, sq.shape)

    for j in range(1, T):
        remote(sq, sq_in.at[j - 1], sq_send, sq_recv.at[j - 1], tp_peer(j)).start()

    def far_first(i):
        half = (i + 1) // 2
        return S // 2 + half * (2 * lax.rem(i, 2) - 1)

    total = as_row
    for j in range(1, T):
        drain(sq_in.at[j - 1], sq_recv.at[j - 1])
        total = total + sq_in[j - 1][0:1, :]
    squares = jnp.sum(jnp.where(spread, total, 0.0), axis=1, keepdims=True)
    inverse = lax.rsqrt(squares * (1.0 / (width * T)) + norm_epsilon)
    normed[...] = (values * inverse).astype(bf16)
    slot_row = iota((S * MAIN, rows), 0).astype(f32)
    placing = ones_where((slot_row == main_row[0]) | (slot_row == main_row[1]))
    for c in range(chunks):
        y = dot(placing, normed[:, c * LANES : (c + 1) * LANES])
        x[:, c] = y.reshape(S, MAIN, LANES).astype(bf16)
    y = jnp.zeros((S * MAIN, LANES), f32)
    for c in range(chunks):
        here = slot_row - float(TAIL * c)
        placing = ones_where((here == tail_row[0]) | (here == tail_row[1]))
        y = y + dot(placing, normed[:, c * LANES : (c + 1) * LANES])
    x[:, chunks] = y.reshape(S, MAIN, LANES).astype(bf16)

    def ship_after(q, c):
        pl.semaphore_wait(ready.at[q], 1)

        @pl.when(mine)
        def _():
            ship(q)

        return c

    lax.fori_loop(place_of + 1, S, ship_after, 0)

    pltpu.make_async_copy(x.at[0], gx.at[tp, 0], d_recv.at[0]).start()

    def dispatch(i, c):
        r = far_first(i)
        d = S - r
        remote(x.at[r], gx.at[tp, d], d_send, d_recv.at[d // rs], fs_peer(r)).start()
        return c

    lax.fori_loop(0, S - 1, dispatch, 0)

    def ranges_of(p):
        return (PAIRS - 1 - p, PAIRS + p)

    def forward(p):
        for q in ranges_of(p):
            part = pl.ds(q * rs, rs)
            drain(gx.at[tp, part], d_recv.at[q])
            for j in range(1, T):
                remote(gx.at[tp, part], gx.at[tp, part], xf_send, x_recv.at[p], tp_peer(j)).start()

    drain(w_group, w_recv)
    for j in range(1, G):
        remote(w_group, w_group, y_send, y_recv.at[j - 1], grp_peer(j)).start()
    forward(0)
    for j in range(1, G):
        other = lax.rem(grp + G - j, G)
        drain(w.at[:, :, other // R, lax.rem(other, R)], y_recv.at[j - 1])
    share = S // T // Q
    pltpu.make_async_copy(w.at[2, pl.ds(tp * share, share)], dx.at[tp], dx_recv).start()
    for j in range(1, T):
        there = lax.rem(tp + j, T)
        remote(w.at[2, pl.ds(there * share, share)], dx.at[tp], dx_send, dx_recv, tp_peer(j)).start()
    outs = (out_gate, out_up, out_down)
    for a, ref in enumerate(outs):
        pltpu.make_async_copy(w.at[a], ref, out_sem.at[a]).start()
    wgu[:, :LANES] = tall(w[0])
    wgu[:, LANES:] = tall(w[1])
    drain(dx, dx_recv)
    for j in range(T):
        wd[:, j * LANES : (j + 1) * LANES] = tall(dx[j])

    half = rs * MAIN
    n_main, n_tail = 2 * half, 2 * rs * TAIL
    q_of = iota((n_tail, n_main), 0)
    tail_home = (q_of >> 1) * MAIN + (q_of & 1)
    picks = [ones_where(iota((n_tail, n_main), 1) == tail_home + TAIL * c) for c in range(chunks)]
    q_of = iota((n_main, n_tail), 1)
    tail_home = (q_of >> 1) * MAIN + (q_of & 1)
    puts = [ones_where(iota((n_main, n_tail), 0) == tail_home + TAIL * c) for c in range(chunks)]

    def first_half(p):
        drain(gx.at[pl.ds(0, T - 1), pl.ds(0, 2 * rs)], x_recv.at[p])
        for j in range(T):
            for s, q in enumerate(ranges_of(p)):
                part = slice(q * rs, (q + 1) * rs)
                for c in range(chunks):
                    k = j * chunks + c
                    lhs[s * half : (s + 1) * half, k * LANES : (k + 1) * LANES] = flat(gx[j, part, c]).astype(bf16)
            tails = jnp.concatenate(
                [flat(gx[j, q * rs : (q + 1) * rs, chunks]) for q in ranges_of(p)], axis=0
            ).astype(bf16)
            for c in range(chunks):
                k = j * chunks + c
                lhs[n_main:, k * LANES : (k + 1) * LANES] = dot(picks[c], tails).astype(bf16)
        both = dot(lhs[...], wgu[...])
        gate, up = both[:, :LANES], both[:, LANES:]
        hb[p, tp] = (gate / (1.0 + jnp.exp(-gate)) * up).astype(bf16)
        for j in range(1, T):
            remote(hb.at[p, tp], hb.at[p, tp], h_send, h_recv.at[p], tp_peer(j)).start()

    def can_wait(to):
        low, high = jnp.minimum(me, to), jnp.maximum(me, to)
        return (high - low > S // 2) & (low >= S * 2 // 8)

    def send_back(d):
        back = lax.rem(S - d, S)
        remote(ob.at[d], ret.at[back], r_send, r_recv.at[back // rs], fs_peer(d)).start()

    def second_half(p):
        drain(hb.at[p, pl.ds(0, T - 1)], h_recv.at[p])
        hidden = jnp.concatenate([hb[p, j] for j in range(T)], axis=1)
        o = dot(hidden, wd[...], ((1,), (1,)))
        y = jnp.zeros((n_main, LANES), f32)
        for c in range(chunks):
            lanes = slice(c * LANES, (c + 1) * LANES)
            y = y + dot(puts[c], o[n_main:, lanes].astype(bf16))
        for s, q in enumerate(ranges_of(p)):
            part = slice(q * rs, (q + 1) * rs)
            for c in range(chunks):
                lanes = slice(c * LANES, (c + 1) * LANES)
                ob[part, c] = o[s * half : (s + 1) * half, lanes].reshape(rs, MAIN, LANES).astype(bf16)
            ob[part, chunks] = y[s * half : (s + 1) * half].reshape(rs, MAIN, LANES).astype(bf16)
        near, far = ranges_of(p)

        last = rs if near else rs - 1

        def send(i, c):
            for d in (far * rs + i, near * rs + rs - 1 - i):

                @pl.when(jnp.logical_not(can_wait(lax.rem(me + d, S))))
                def _():
                    send_back(d)

            return c

        lax.fori_loop(0, last, send, 0)
        if not near:

            send_back(S - 1)

            pltpu.make_async_copy(ob.at[0], ret.at[0], r_recv.at[0]).start()

    for p in range(PAIRS):
        first_half(p)
        if p + 1 < PAIRS:
            forward(p + 1)
        second_half(p)

    def send_late(i, c):
        d = far_first(i)

        @pl.when(can_wait(lax.rem(me + d, S)))
        def _():
            send_back(d)

        return c

    lax.fori_loop(0, S - 1, send_late, 0)

    acc[...] = jnp.zeros_like(acc)
    for p in range(PAIRS):
        near, far = ranges_of(p)
        lane = iota((rows, n_main), 1)
        home = jnp.where(lane < half, lane + near * half, lane + (far - 1) * half).astype(f32)
        for q in (near, far):
            drain(ret.at[pl.ds(q * rs, rs)], r_recv.at[q])

        def piece(c):
            return jnp.concatenate(
                [flat(ret[q * rs : (q + 1) * rs, c]) for q in (near, far)], axis=0
            ).astype(bf16)

        tails = piece(chunks)
        for c in range(chunks):
            lanes = slice(c * LANES, (c + 1) * LANES)
            values = piece(c)
            for k in range(2):
                acc[k, :, lanes] += dot(ones_where(home == main[k]), values) + dot(
                    ones_where(home == tail[k] + float(TAIL * c)), tails
                )
    weight = [as_column(route_w[k : k + 1, :]) for k in range(2)]
    out_moe[...] = (weight[0] * acc[0] + weight[1] * acc[1]).astype(bf16)

    drain(sq_in, sq_send)

    @pl.when(mine)
    def _():
        drain(ws.at[pl.ds(1, S - 1)], w_send)

    drain(x.at[pl.ds(1, S - 1)], d_send)
    for j in range(1, G):
        drain(w_group, y_send)
    drain(gx.at[pl.ds(0, T - 1)], xf_send)
    drain(dx.at[pl.ds(0, T - 1)], dx_send)
    drain(hb.at[:, pl.ds(0, T - 1)], h_send)
    drain(ob.at[pl.ds(1, S - 1)], r_send)
    for a, ref in enumerate(outs):
        drain(w.at[a], out_sem.at[a])


def settle(*refs):
    n = (len(refs) - 2) // 3
    sources, targets, held = refs[:n], refs[n : 2 * n], refs[2 * n : 3 * n]
    in_sem, out_sem = refs[3 * n :]
    for i in range(n):
        pltpu.make_async_copy(sources[i], held[i], in_sem.at[i]).start()
    for i in range(n):
        pltpu.make_async_copy(sources[i], held[i], in_sem.at[i]).wait()
        pltpu.make_async_copy(held[i], targets[i], out_sem.at[i]).start()
    for i in range(n):
        pltpu.make_async_copy(held[i], targets[i], out_sem.at[i]).wait()


def local(shards, columns, groups, tokens, route_ids, route_weights, norm_gain, gate_m, up_m, down_m):
    S, T, G = shards, columns, groups
    rows, width = tokens.shape
    depth = gate_m.shape[1]
    chunks = width // LANES
    rs = S // RANGES
    padded = -(-rows // LANES) * LANES
    n_rows = 2 * rs * (MAIN + TAIL)
    vmem = pl.BlockSpec(memory_space=pltpu.VMEM)
    anywhere = pl.BlockSpec(memory_space=pl.ANY)
    dma = pltpu.SemaphoreType.DMA
    block = (chunks + 1, MAIN, LANES)
    Q, R = parts_of(G)
    strip = depth // R
    served = jax.ShapeDtypeStruct((S // Q, Q, R, strip, LANES), bf16)
    outs = pl.pallas_call(
        functools.partial(kernel, S, T, G),
        out_shape=(served, served, served, jax.ShapeDtypeStruct((rows, width), bf16)),
        in_specs=[vmem] * 4 + [anywhere] * 3,
        out_specs=(anywhere, anywhere, anywhere, vmem),
        scratch_shapes=[
            pltpu.VMEM((3, S, strip, LANES), f32),
            pltpu.VMEM((S, 3, strip, LANES), bf16),
            pltpu.VMEM((3, S // Q, Q, R, strip, LANES), bf16),
            pltpu.VMEM((S * depth, 2 * LANES), bf16),
            pltpu.VMEM((width, T * LANES), bf16),
            pltpu.VMEM((T, S // T // Q, Q, R, strip, LANES), bf16),
            pltpu.VMEM((rows, width), bf16),
            pltpu.VMEM((S, *block), bf16),
            pltpu.VMEM((T, S, *block), bf16),
            pltpu.VMEM((n_rows, T * width), bf16),
            pltpu.VMEM((PAIRS, T, n_rows, LANES), bf16),
            pltpu.VMEM((S, *block), bf16),
            pltpu.VMEM((S, *block), bf16),
            pltpu.VMEM((2, rows, width), f32),
            pltpu.VMEM((MAIN, padded), f32),
            pltpu.VMEM((T - 1, MAIN, padded), f32),
            pltpu.SemaphoreType.REGULAR((S,)),
            dma((3,)), dma((3,)), dma, dma, dma, dma((max(G - 1, 1),)), dma, dma((T - 1,)), dma, dma((RANGES,)),
            dma, dma((PAIRS,)), dma, dma, dma, dma((PAIRS,)), dma, dma((RANGES,)),
        ],
        compiler_params=pltpu.CompilerParams(collective_id=0, has_side_effects=True),
    )(tokens, route_ids.T, route_weights.T, norm_gain[None, :], gate_m, up_m, down_m)
    outs = [o.reshape(1, S * depth, LANES) for o in outs[:3]] + [outs[3]]
    return pl.pallas_call(
        settle,
        out_shape=tuple(jax.ShapeDtypeStruct(o.shape, o.dtype) for o in outs),
        in_specs=[anywhere] * len(outs),
        out_specs=(anywhere,) * len(outs),
        scratch_shapes=[pltpu.VMEM(o.shape, o.dtype) for o in outs] + [dma((len(outs),)), dma((len(outs),))],
    )(*outs)


def solution(mesh):
    placed = (
        P(GRP_FS, "tp"), P(GRP_FS, None), P(GRP_FS, None), P("fs"),
        P(None, "fs", "tp"), P(None, "fs", "tp"), P(None, "fs", "tp"),
    )
    return jax.shard_map(
        functools.partial(local, mesh.shape["fs"], mesh.shape["tp"], mesh.shape["grp"]),
        mesh=mesh,
        in_specs=placed,
        out_specs=(P(GRP_FS, None, "tp"), P(GRP_FS, None, "tp"), P(GRP_FS, None, "tp"), P(GRP_FS, "tp")),
        check_vma=False,
    )
```

```python
import functools

import jax
import jax.numpy as jnp
from jax import lax
from jax.experimental import pallas as pl
from jax.experimental.pallas import tpu as pltpu
from jax.sharding import PartitionSpec as P

MESH = pl.DeviceIdType.MESH
GRP_FS = ("grp", "fs")
norm_epsilon = 1e-06

LANES = 128
MAIN = 8
TAIL = 2
RANGES = 8
PAIRS = RANGES // 2

f32, bf16 = jnp.float32, jnp.bfloat16


def iota(shape, dim):
    return lax.broadcasted_iota(jnp.int32, shape, dim)


def ones_where(mask):
    return jnp.where(mask, 1.0, 0.0).astype(bf16)


def drain(ref, sem):
    pltpu.make_async_copy(ref, ref, sem).wait()


def parts_of(groups):
    rows = min(groups, 4)
    return groups // rows, rows


def tall(blocks):
    if blocks.shape[-2] % 16:
        return blocks.astype(f32).reshape(-1, LANES).astype(bf16)
    return blocks.reshape(-1, LANES)


def dot(a, b, dims=((1,), (0,))):
    return lax.dot_general(a, b, (dims, ((), ())), preferred_element_type=f32)


def flat(tiles):
    n = tiles.shape[0]
    return tiles.astype(f32).reshape(n * MAIN, LANES)


def kernel(
    shards, columns, groups,
    tok, ids, route_w, gain, gate_m, up_m, down_m,
    out_gate, out_up, out_down, out_moe,
    stage, ws, w, wgu, wd, dx, normed, x, gx, lhs, hb, ob, ret, acc, sq, sq_in, ready,
    stage_sem, out_sem, w_send, w_recv, y_send, y_recv, sq_send, sq_recv, d_send, d_recv,
    xf_send, x_recv, dx_send, dx_recv, h_send, h_recv, r_send, r_recv,
):
    S, T, G = shards, columns, groups
    me, tp, grp = lax.axis_index("fs"), lax.axis_index("tp"), lax.axis_index("grp")
    rs = S // RANGES
    rows, width = tok.shape
    chunks = width // LANES
    depth = gate_m.shape[1]
    Q, R = parts_of(G)
    strip = depth // R
    turn, part = grp // R, lax.rem(grp, R)
    mine = lax.rem(me, Q) == turn

    def fs_peer(r):
        return {"fs": lax.rem(me + r, S)}

    def tp_peer(j):
        return {"tp": lax.rem(tp + j, T)}

    def grp_peer(j):
        return {"grp": lax.rem(grp + j, G)}

    def remote(src, dst, send, recv, peer):
        return pltpu.make_async_remote_copy(
            src_ref=src, dst_ref=dst, send_sem=send, recv_sem=recv, device_id=peer, device_id_type=MESH
        )

    @pl.when(mine)
    def _():
        for a, ref in enumerate((gate_m, up_m, down_m)):
            pltpu.make_async_copy(ref.at[:, pl.ds(part * strip, strip)], stage.at[a], stage_sem.at[a]).start()

    place_of = lax.rem(me + S - 1, S)

    def placed_at(q):
        return {"fs": lax.rem(q + 1, S)}

    barrier = pltpu.get_barrier_semaphore()

    def greet(q, c):
        pl.semaphore_signal(barrier, inc=1, device_id=placed_at(q), device_id_type=MESH)
        return c

    lax.fori_loop(place_of + 1, S, greet, 0)
    for j in range(1, T):
        pl.semaphore_signal(barrier, inc=1, device_id=tp_peer(j), device_id_type=MESH)
    for j in range(1, G):
        pl.semaphore_signal(barrier, inc=1, device_id=grp_peer(j), device_id_type=MESH)
    pl.semaphore_wait(barrier, place_of + (T - 1) + (G - 1))

    def report(q, c):
        pl.semaphore_signal(ready.at[place_of], inc=1, device_id=placed_at(q), device_id_type=MESH)
        return c

    lax.fori_loop(0, place_of, report, 0)

    w_mine = w.at[:, me // Q, lax.rem(me, Q), part]
    w_group = w.at[:, :, turn, part]

    def ship(q):
        r = lax.rem(q + 1 + S - me, S)
        remote(ws.at[r], w_mine, w_send, w_recv, placed_at(q)).start()

    @pl.when(mine)
    def _():
        for a in range(3):
            drain(stage.at[a], stage_sem.at[a])
        eye = iota((strip, depth), 0) + part * strip == iota((strip, depth), 1)
        column = jnp.sum(jnp.where(eye, gain[...], 0.0), axis=1, keepdims=True)
        scale = jnp.broadcast_to(column, (strip, LANES))

        def convert(r, c):
            e = lax.rem(me + r, S)
            ws[r, 0] = (stage[0, e] * scale).astype(bf16)
            ws[r, 1] = (stage[1, e] * scale).astype(bf16)
            ws[r, 2] = stage[2, e].astype(bf16)
            return c

        lax.fori_loop(0, S, convert, 0)
        pltpu.make_async_copy(ws.at[0], w_mine, w_recv).start()

        def ship_before(i, c):
            ship(i)
            return c

        lax.fori_loop(0, place_of, ship_before, 0)

    diagonal = iota((rows, rows), 0) == iota((rows, rows), 1)

    def as_column(row):
        return jnp.sum(jnp.where(diagonal, row, 0.0), axis=1, keepdims=True)

    expert_lane = iota((rows, S), 1).astype(f32)
    rel = []
    for k in range(2):
        r = ids[k : k + 1, :] - me
        rel.append(as_column(jnp.where(r < 0, r + S, r).astype(f32)))
    named = [jnp.where(r == expert_lane, 1.0, 0.0) for r in rel]
    earlier = ones_where(iota((rows, rows), 0) > iota((rows, rows), 1))
    before = dot(earlier, (named[0] + named[1]).astype(bf16))
    main, tail, main_row, tail_row = [], [], [], []
    for k in range(2):
        place = jnp.sum(before * named[k], axis=1, keepdims=True)
        base = rel[k] * MAIN
        main.append(jnp.where(place < MAIN, base + place, -1.0))
        tail.append(jnp.where(place < MAIN, -64.0, base + (place - MAIN)))
        main_row.append(jnp.sum(jnp.where(diagonal, main[k], 0.0), axis=0, keepdims=True))
        tail_row.append(jnp.sum(jnp.where(diagonal, tail[k], 0.0), axis=0, keepdims=True))

    values = tok[...].astype(f32)
    squares = jnp.sum(values * values, axis=1, keepdims=True)
    padded = sq.shape[1]
    spread = iota((rows, padded), 0) == iota((rows, padded), 1)
    as_row = jnp.sum(jnp.where(spread, squares, 0.0), axis=0, keepdims=True)
    sq[...] = jnp.broadcast_to(as_row, sq.shape)

    for j in range(1, T):
        remote(sq, sq_in.at[j - 1], sq_send, sq_recv.at[j - 1], tp_peer(j)).start()

    def far_first(i):
        half = (i + 1) // 2
        return S // 2 + half * (2 * lax.rem(i, 2) - 1)

    total = as_row
    for j in range(1, T):
        drain(sq_in.at[j - 1], sq_recv.at[j - 1])
        total = total + sq_in[j - 1][0:1, :]
    squares = jnp.sum(jnp.where(spread, total, 0.0), axis=1, keepdims=True)
    inverse = lax.rsqrt(squares * (1.0 / (width * T)) + norm_epsilon)
    normed[...] = (values * inverse).astype(bf16)
    slot_row = iota((S * MAIN, rows), 0).astype(f32)
    placing = ones_where((slot_row == main_row[0]) | (slot_row == main_row[1]))
    for c in range(chunks):
        y = dot(placing, normed[:, c * LANES : (c + 1) * LANES])
        x[:, c] = y.reshape(S, MAIN, LANES).astype(bf16)
    y = jnp.zeros((S * MAIN, LANES), f32)
    for c in range(chunks):
        here = slot_row - float(TAIL * c)
        placing = ones_where((here == tail_row[0]) | (here == tail_row[1]))
        y = y + dot(placing, normed[:, c * LANES : (c + 1) * LANES])
    x[:, chunks] = y.reshape(S, MAIN, LANES).astype(bf16)

    def ship_after(q, c):
        pl.semaphore_wait(ready.at[q], 1)

        @pl.when(mine)
        def _():
            ship(q)

        return c

    lax.fori_loop(place_of + 1, S, ship_after, 0)

    pltpu.make_async_copy(x.at[0], gx.at[tp, 0], d_recv.at[0]).start()

    def dispatch(i, c):
        r = far_first(i)
        d = S - r
        remote(x.at[r], gx.at[tp, d], d_send, d_recv.at[d // rs], fs_peer(r)).start()
        return c

    lax.fori_loop(0, S - 1, dispatch, 0)

    def ranges_of(p):
        return (PAIRS - 1 - p, PAIRS + p)

    def forward(p):
        for q in ranges_of(p):
            part = pl.ds(q * rs, rs)
            drain(gx.at[tp, part], d_recv.at[q])
            for j in range(1, T):
                remote(gx.at[tp, part], gx.at[tp, part], xf_send, x_recv.at[p], tp_peer(j)).start()

    drain(w_group, w_recv)
    for j in range(1, G):
        remote(w_group, w_group, y_send, y_recv.at[j - 1], grp_peer(j)).start()
    forward(0)
    for j in range(1, G):
        other = lax.rem(grp + G - j, G)
        drain(w.at[:, :, other // R, lax.rem(other, R)], y_recv.at[j - 1])
    share = S // T // Q
    pltpu.make_async_copy(w.at[2, pl.ds(tp * share, share)], dx.at[tp], dx_recv).start()
    for j in range(1, T):
        there = lax.rem(tp + j, T)
        remote(w.at[2, pl.ds(there * share, share)], dx.at[tp], dx_send, dx_recv, tp_peer(j)).start()
    outs = (out_gate, out_up, out_down)
    for a, ref in enumerate(outs):
        pltpu.make_async_copy(w.at[a], ref, out_sem.at[a]).start()
    wgu[:, :LANES] = tall(w[0])
    wgu[:, LANES:] = tall(w[1])
    drain(dx, dx_recv)
    for j in range(T):
        wd[:, j * LANES : (j + 1) * LANES] = tall(dx[j])

    half = rs * MAIN
    n_main, n_tail = 2 * half, 2 * rs * TAIL
    q_of = iota((n_tail, n_main), 0)
    tail_home = (q_of >> 1) * MAIN + (q_of & 1)
    picks = [ones_where(iota((n_tail, n_main), 1) == tail_home + TAIL * c) for c in range(chunks)]
    q_of = iota((n_main, n_tail), 1)
    tail_home = (q_of >> 1) * MAIN + (q_of & 1)
    puts = [ones_where(iota((n_main, n_tail), 0) == tail_home + TAIL * c) for c in range(chunks)]

    def first_half(p):
        drain(gx.at[pl.ds(0, T - 1), pl.ds(0, 2 * rs)], x_recv.at[p])
        for j in range(T):
            for s, q in enumerate(ranges_of(p)):
                part = slice(q * rs, (q + 1) * rs)
                for c in range(chunks):
                    k = j * chunks + c
                    lhs[s * half : (s + 1) * half, k * LANES : (k + 1) * LANES] = flat(gx[j, part, c]).astype(bf16)
            tails = jnp.concatenate(
                [flat(gx[j, q * rs : (q + 1) * rs, chunks]) for q in ranges_of(p)], axis=0
            ).astype(bf16)
            for c in range(chunks):
                k = j * chunks + c
                lhs[n_main:, k * LANES : (k + 1) * LANES] = dot(picks[c], tails).astype(bf16)
        both = dot(lhs[...], wgu[...])
        gate, up = both[:, :LANES], both[:, LANES:]
        hb[p, tp] = (gate / (1.0 + jnp.exp(-gate)) * up).astype(bf16)
        for j in range(1, T):
            remote(hb.at[p, tp], hb.at[p, tp], h_send, h_recv.at[p], tp_peer(j)).start()

    def can_wait(to):
        low, high = jnp.minimum(me, to), jnp.maximum(me, to)
        return (high - low > S // 2) & (low >= S * 2 // 8)

    def send_back(d):
        back = lax.rem(S - d, S)
        remote(ob.at[d], ret.at[back], r_send, r_recv.at[back // rs], fs_peer(d)).start()

    def second_half(p):
        drain(hb.at[p, pl.ds(0, T - 1)], h_recv.at[p])
        hidden = jnp.concatenate([hb[p, j] for j in range(T)], axis=1)
        o = dot(hidden, wd[...], ((1,), (1,)))
        y = jnp.zeros((n_main, LANES), f32)
        for c in range(chunks):
            lanes = slice(c * LANES, (c + 1) * LANES)
            y = y + dot(puts[c], o[n_main:, lanes].astype(bf16))
        for s, q in enumerate(ranges_of(p)):
            part = slice(q * rs, (q + 1) * rs)
            for c in range(chunks):
                lanes = slice(c * LANES, (c + 1) * LANES)
                ob[part, c] = o[s * half : (s + 1) * half, lanes].reshape(rs, MAIN, LANES).astype(bf16)
            ob[part, chunks] = y[s * half : (s + 1) * half].reshape(rs, MAIN, LANES).astype(bf16)
        near, far = ranges_of(p)

        last = rs if near else rs - 1

        def send(i, c):
            for d in (far * rs + i, near * rs + rs - 1 - i):

                @pl.when(jnp.logical_not(can_wait(lax.rem(me + d, S))))
                def _():
                    send_back(d)

            return c

        lax.fori_loop(0, last, send, 0)
        if not near:

            send_back(S - 1)

            pltpu.make_async_copy(ob.at[0], ret.at[0], r_recv.at[0]).start()

    for p in range(PAIRS):
        first_half(p)
        if p + 1 < PAIRS:
            forward(p + 1)
        second_half(p)

    def send_late(i, c):
        d = far_first(i)

        @pl.when(can_wait(lax.rem(me + d, S)))
        def _():
            send_back(d)

        return c

    lax.fori_loop(0, S - 1, send_late, 0)

    acc[...] = jnp.zeros_like(acc)
    for p in range(PAIRS):
        near, far = ranges_of(p)
        lane = iota((rows, n_main), 1)
        home = jnp.where(lane < half, lane + near * half, lane + (far - 1) * half).astype(f32)
        for q in (near, far):
            drain(ret.at[pl.ds(q * rs, rs)], r_recv.at[q])

        def piece(c):
            return jnp.concatenate(
                [flat(ret[q * rs : (q + 1) * rs, c]) for q in (near, far)], axis=0
            ).astype(bf16)

        tails = piece(chunks)
        for c in range(chunks):
            lanes = slice(c * LANES, (c + 1) * LANES)
            values = piece(c)
            for k in range(2):
                acc[k, :, lanes] += dot(ones_where(home == main[k]), values) + dot(
                    ones_where(home == tail[k] + float(TAIL * c)), tails
                )
    weight = [as_column(route_w[k : k + 1, :]) for k in range(2)]
    out_moe[...] = (weight[0] * acc[0] + weight[1] * acc[1]).astype(bf16)

    drain(sq_in, sq_send)

    @pl.when(mine)
    def _():
        drain(ws.at[pl.ds(1, S - 1)], w_send)

    drain(x.at[pl.ds(1, S - 1)], d_send)
    for j in range(1, G):
        drain(w_group, y_send)
    drain(gx.at[pl.ds(0, T - 1)], xf_send)
    drain(dx.at[pl.ds(0, T - 1)], dx_send)
    drain(hb.at[:, pl.ds(0, T - 1)], h_send)
    drain(ob.at[pl.ds(1, S - 1)], r_send)
    for a, ref in enumerate(outs):
        drain(w.at[a], out_sem.at[a])


def settle(*refs):
    n = (len(refs) - 2) // 3
    sources, targets, held = refs[:n], refs[n : 2 * n], refs[2 * n : 3 * n]
    in_sem, out_sem = refs[3 * n :]
    for i in range(n):
        pltpu.make_async_copy(sources[i], held[i], in_sem.at[i]).start()
    for i in range(n):
        pltpu.make_async_copy(sources[i], held[i], in_sem.at[i]).wait()
        pltpu.make_async_copy(held[i], targets[i], out_sem.at[i]).start()
    for i in range(n):
        pltpu.make_async_copy(held[i], targets[i], out_sem.at[i]).wait()


def local(shards, columns, groups, tokens, route_ids, route_weights, norm_gain, gate_m, up_m, down_m):
    S, T, G = shards, columns, groups
    rows, width = tokens.shape
    depth = gate_m.shape[1]
    chunks = width // LANES
    rs = S // RANGES
    padded = -(-rows // LANES) * LANES
    n_rows = 2 * rs * (MAIN + TAIL)
    vmem = pl.BlockSpec(memory_space=pltpu.VMEM)
    anywhere = pl.BlockSpec(memory_space=pl.ANY)
    dma = pltpu.SemaphoreType.DMA
    block = (chunks + 1, MAIN, LANES)
    Q, R = parts_of(G)
    strip = depth // R
    served = jax.ShapeDtypeStruct((S // Q, Q, R, strip, LANES), bf16)
    outs = pl.pallas_call(
        functools.partial(kernel, S, T, G),
        out_shape=(served, served, served, jax.ShapeDtypeStruct((rows, width), bf16)),
        in_specs=[vmem] * 4 + [anywhere] * 3,
        out_specs=(anywhere, anywhere, anywhere, vmem),
        scratch_shapes=[
            pltpu.VMEM((3, S, strip, LANES), f32),
            pltpu.VMEM((S, 3, strip, LANES), bf16),
            pltpu.VMEM((3, S // Q, Q, R, strip, LANES), bf16),
            pltpu.VMEM((S * depth, 2 * LANES), bf16),
            pltpu.VMEM((width, T * LANES), bf16),
            pltpu.VMEM((T, S // T // Q, Q, R, strip, LANES), bf16),
            pltpu.VMEM((rows, width), bf16),
            pltpu.VMEM((S, *block), bf16),
            pltpu.VMEM((T, S, *block), bf16),
            pltpu.VMEM((n_rows, T * width), bf16),
            pltpu.VMEM((PAIRS, T, n_rows, LANES), bf16),
            pltpu.VMEM((S, *block), bf16),
            pltpu.VMEM((S, *block), bf16),
            pltpu.VMEM((2, rows, width), f32),
            pltpu.VMEM((MAIN, padded), f32),
            pltpu.VMEM((T - 1, MAIN, padded), f32),
            pltpu.SemaphoreType.REGULAR((S,)),
            dma((3,)), dma((3,)), dma, dma, dma, dma((max(G - 1, 1),)), dma, dma((T - 1,)), dma, dma((RANGES,)),
            dma, dma((PAIRS,)), dma, dma, dma, dma((PAIRS,)), dma, dma((RANGES,)),
        ],
        compiler_params=pltpu.CompilerParams(collective_id=0, has_side_effects=True),
    )(tokens, route_ids.T, route_weights.T, norm_gain[None, :], gate_m, up_m, down_m)
    outs = [o.reshape(1, S * depth, LANES) for o in outs[:3]] + [outs[3]]
    return pl.pallas_call(
        settle,
        out_shape=tuple(jax.ShapeDtypeStruct(o.shape, o.dtype) for o in outs),
        in_specs=[anywhere] * len(outs),
        out_specs=(anywhere,) * len(outs),
        scratch_shapes=[pltpu.VMEM(o.shape, o.dtype) for o in outs] + [dma((len(outs),)), dma((len(outs),))],
    )(*outs)


def solution(mesh):
    placed = (
        P(GRP_FS, "tp"), P(GRP_FS, None), P(GRP_FS, None), P("fs"),
        P(None, "fs", "tp"), P(None, "fs", "tp"), P(None, "fs", "tp"),
    )
    return jax.shard_map(
        functools.partial(local, mesh.shape["fs"], mesh.shape["tp"], mesh.shape["grp"]),
        mesh=mesh,
        in_specs=placed,
        out_specs=(P(GRP_FS, None, "tp"), P(GRP_FS, None, "tp"), P(GRP_FS, None, "tp"), P(GRP_FS, "tp")),
        check_vma=False,
    )
```
